32 devices in a mesh: grp: 2 (over x), ep: 8 (over z, y), tp: 2 (over core).
Axes of the slice: x: 2, y: 2, z: 4, core: 2. Of those that a mesh axis runs over, the one named last changes fastest.
Arguments:
- tokens: bfloat16 [4096, 2048], P(('grp', 'ep'), 'tp'), parts along dimension 0, may hold values from -40 to 40
- in_gain: float32 [2048], P('tp'), may hold values from 0.1 to 1.9
- route_ids: int32 [4096, 2], P(('grp', 'ep')), parts along dimension 0, may hold values from 0 to 3, all different within a row; in each aligned block of 256 rows (0 to 255, 256 to 511, ...) at most 160 rows name the same one
- route_weights: float32 [4096, 2], P(('grp', 'ep')), parts along dimension 0, may hold values from 0.1 to 1
- w_gate: bfloat16 [8, 2048, 1792], P('ep', None, 'tp'), may hold values from -0.125 to 0.125
- w_up: bfloat16 [8, 2048, 1792], P('ep', None, 'tp'), may hold values from -0.125 to 0.125
- w_down: bfloat16 [8, 1792, 2048], P('ep', 'tp'), may hold values from -1.5 to 1.5
- out_gain: float32 [2048], P('tp'), may hold values from 0.1 to 1.9
Outputs:
- mixed: bfloat16 [4096, 2048], P(('grp', 'ep'), 'tp'), parts along dimension 0
The draws below stay inside these ranges and needn't reach their ends.
There are 2 independent parts, one for each index of `grp`. The reference program is written for one: setup_inputs(seed, part) draws one part's arguments, and reference() takes and returns one part's arrays. A program takes and returns all parts, laid end to end along the dimension named above; an argument that names none is the same for every part. Nothing has to cross between parts.
Inputs may be any that keep to these rules, and one draw needn't show every extreme that they name: `route_ids`: A token's two experts differ. Within each aligned block of 256 tokens no expert is named more than 160 times, and in some blocks some expert is named exactly 160 times.
All inputs are finite; a program needn't handle non-finite values.
Results may differ from the reference program's by a relative error of at most 0.012.
Values may be sent and summed in bfloat16 or wider, within the bound.
No kernel may reach another device: no remote copies, remote signals or barrier semaphores. Data moves between devices by JAX's collectives and lax.ppermute only.
A program may use at most 128 MiB of HBM per device.

```python
import math
import jax
import jax.numpy as jnp
import numpy as np
from jax import lax

D = 2048
FF = 3584
SPAN_EP = 2
TOK_DEV = 256
EXPERTS = 4
CAP = 160
TOKENS = 2048
N_EP = 8


def draw_tokens(key, part):
    key_noise = jax.random.fold_in(key, 11)
    position = jnp.arange(D, dtype=jnp.float32) / (D - 1)
    noise = jnp.clip(jax.random.normal(key_noise, (TOKENS, D), jnp.float32), -6.0, 6.0)
    column_scale = jnp.exp(jnp.log(6.0) * position)
    values = noise * column_scale[None, :]
    return jnp.clip(values, -40.0, 40.0).astype(jnp.bfloat16)


def draw_w_down(key, part):
    key_noise = jax.random.fold_in(key, 21)
    rows = FF // SPAN_EP
    position = jnp.arange(D, dtype=jnp.float32) / (D - 1)
    noise = jnp.clip(jax.random.normal(key_noise, (N_EP, rows, D), jnp.float32), -6.0, 6.0)
    rise = jnp.exp(jnp.log(8.0) * position)
    rise = rise / jnp.sqrt(jnp.mean(rise * rise))
    values = noise * rise[None, None, :] / jnp.sqrt(jnp.float32(FF))
    return jnp.clip(values, -1.5, 1.5).astype(jnp.bfloat16)


def block_scale(key, shape, pieces, least, top_value):
    loudness = 1.0
    for dim, blocks in pieces:
        heights = jax.random.uniform(jax.random.fold_in(jax.random.fold_in(key, 6), dim), (blocks,), jnp.float32, least / len(pieces), top_value / len(pieces))
        loudness = loudness * jnp.repeat(jnp.exp(heights), shape[dim] // blocks).reshape((-1,) + (1,) * (len(shape) - 1 - dim))
    return loudness


def routed_block(rng, own, number, rows, amount, top, bound, slope):
    ranking = jax.random.permutation(rng, amount)
    crowded, common = portions_of(amount, rows * top, bound, slope, True), portions_of(amount, rows * top, bound, slope, False)
    places = jnp.arange(amount)

    def named(lengths, rotation):
        used = int((lengths > 0).sum())
        fixed = max(1, used // 4)
        moved = fixed + (places - fixed + rotation * (used - fixed)) % max(1, amount - fixed)
        return jnp.zeros((amount,), jnp.int32).at[ranking[jnp.where(places < fixed, places, moved)]].set(jnp.asarray(lengths, jnp.int32))

    lengths = jnp.where(number % 4 == 0, named(crowded, number // 4), named(common, number - number // 4 - 1))
    mixed = jax.random.permutation(jax.random.fold_in(own, 3), amount)
    donor, sink = mixed[0:amount // 2 * 2:2], mixed[1:amount // 2 * 2:2]
    room = jnp.minimum(lengths[donor] - 1, bound - lengths[sink]) // 2
    room = jnp.where((donor == ranking[0]) | (sink == ranking[0]) | (lengths[sink] == 0), 0, jnp.maximum(room, 0))
    moved = jax.random.randint(jax.random.fold_in(own, 4), (amount // 2,), 0, 1 << 20) % (room + 1)
    lengths = lengths.at[donor].add(-moved).at[sink].add(moved)
    items = jnp.searchsorted(jnp.cumsum(lengths), jnp.arange(rows * top), side="right").astype(jnp.int32)
    grid = items.reshape(top, rows).T
    grid = grid[jax.random.permutation(jax.random.fold_in(own, 1), rows)]
    rotation = jax.random.randint(jax.random.fold_in(own, 2), (rows, 1), 0, top)
    return jnp.take_along_axis(grid, (jnp.arange(top)[None, :] + rotation) % top, axis=1)


def portions_of(number_of, total, reach, lean, full):
    portions = [(1 << 20) // math.isqrt(grade ** lean) + 1 for grade in range(1, number_of + 1)]
    largest = reach if full else min(reach, max(-(-total // number_of), total * portions[0] // sum(portions)))
    least = 1 if total - largest >= number_of - 1 else 0
    holding, rest = [largest] + [least] * (number_of - 1), total - largest - least * (number_of - 1)
    while rest > 0:
        movable = [i for i in range(1, number_of) if holding[i] < largest] or [i for i in range(1, number_of) if holding[i] < reach]
        pool, left = sum([portions[i] for i in movable]), rest
        for i in movable:
            more = min(reach - holding[i], max(1, left * portions[i] // pool), rest)
            holding[i] = holding[i] + more
            rest = rest - more
    return np.array(holding)


def centred(key, extent, scale, most, cuts=(), kind=jnp.bfloat16):
    values = scale * jax.random.normal(key, extent, jnp.float32)
    if cuts:
        values = values * block_scale(key, extent, cuts, -0.22, 0.18)
    return jnp.clip(values, -most, most).astype(kind)


def setup_inputs(seed: int = 0, part: int = 0) -> dict:
    seeds = jax.random.split(jax.random.key(seed), 9)
    part_splits = jax.random.split(jax.random.fold_in(seeds[8], part), 9)
    tokens = draw_tokens(jax.random.fold_in(jax.random.fold_in(seeds[8], part), 71), part)
    in_gain = jnp.clip(1.0 + 0.18 * jax.random.normal(seeds[1], (D,), jnp.float32), 0.1, 1.9)
    route_ids_keys = jax.random.split(jax.random.fold_in(part_splits[2], 1), TOKENS // TOK_DEV)
    route_ids_turns = jax.random.permutation(jax.random.fold_in(part_splits[2], 3), TOKENS // TOK_DEV)
    route_ids = jax.vmap(lambda own, number: routed_block(jax.random.fold_in(part_splits[2], 2), own, number, TOK_DEV, EXPERTS, 2, CAP, 2))(route_ids_keys, route_ids_turns).reshape((TOKENS, 2))
    route_weights = jnp.clip(0.1 + 0.9 * jax.random.uniform(part_splits[3], (TOKENS, 2), jnp.float32) ** block_scale(part_splits[3], (TOKENS, 2), ((0, 8),), -0.2, 0.2), 0.1, 1.0)
    w_gate = centred(seeds[4], (N_EP, D, FF // SPAN_EP), D ** -0.5, 0.125, ((0, 8), (2, 2)))
    w_up = centred(seeds[5], (N_EP, D, FF // SPAN_EP), D ** -0.5, 0.125, ((0, 8), (2, 2)))
    w_down = draw_w_down(jax.random.fold_in(seeds[8], 71), part)
    out_gain = jnp.clip(1.0 + 0.18 * jax.random.normal(seeds[7], (D,), jnp.float32), 0.1, 1.9)
    return {"tokens": tokens, "in_gain": in_gain, "route_ids": route_ids, "route_weights": route_weights, "w_gate": w_gate, "w_up": w_up, "w_down": w_down, "out_gain": out_gain}


EPS = 1e-06

def reference(tokens, in_gain, route_ids, route_weights, w_gate, w_up, w_down, out_gain):
    experts = N_EP // SPAN_EP
    quarter = FF // (2 * SPAN_EP)
    tok_float = tokens.astype(jnp.float32)
    inv_first = lax.rsqrt(lax.optimization_barrier(jnp.mean(tok_float * tok_float, axis=1, keepdims=True)) + EPS)
    normed = (tok_float * inv_first * in_gain[None, :]).astype(jnp.bfloat16)
    route_flat = route_ids.reshape(N_EP, TOK_DEV * 2).astype(jnp.int32)
    onehot = (route_flat[:, :, None] == jnp.arange(experts, dtype=jnp.int32)[None, None, :]).astype(jnp.int32)
    before = jnp.cumsum(onehot, axis=1) - onehot
    slot_of = lax.optimization_barrier(jnp.sum(before * onehot, axis=2)).astype(jnp.int32)
    target = (route_flat * CAP + slot_of).astype(jnp.int32)
    copies = jnp.repeat(normed.reshape(N_EP, TOK_DEV, D), 2, axis=1)
    blocks = jnp.arange(N_EP, dtype=jnp.int32)[:, None]
    buffers = jnp.zeros((N_EP, experts * CAP, D), jnp.bfloat16).at[blocks, target].set(copies)
    buffers = buffers.reshape(N_EP, experts, CAP, D).transpose(1, 0, 2, 3)
    gate_stack = w_gate.reshape(experts, SPAN_EP, D, FF // SPAN_EP)
    up_stack = w_up.reshape(experts, SPAN_EP, D, FF // SPAN_EP)
    down_stack = w_down.reshape(experts, SPAN_EP, FF // SPAN_EP, D)

    def one_expert(inputs):
        expert_rows, gate_w, up_w, down_w = inputs
        tok_rows = expert_rows.reshape(N_EP * CAP, D)
        accum_sum = jnp.zeros((N_EP * CAP, D), jnp.float32)
        for segment in range(SPAN_EP):
            gate_act = jnp.dot(tok_rows, gate_w[segment], preferred_element_type=jnp.float32)
            up_act = jnp.dot(tok_rows, up_w[segment], preferred_element_type=jnp.float32)
            hidden = (jax.nn.silu(gate_act) * up_act).astype(jnp.bfloat16)
            pair_sum = jnp.zeros((N_EP * CAP, D), jnp.float32)
            for core_half in range(2):
                quarter_part = jnp.dot(hidden[:, core_half * quarter:(core_half + 1) * quarter], down_w[segment, core_half * quarter:(core_half + 1) * quarter], preferred_element_type=jnp.float32)
                pair_sum = pair_sum + lax.optimization_barrier(quarter_part.astype(jnp.bfloat16)).astype(jnp.float32)
            accum_sum = accum_sum + lax.optimization_barrier(pair_sum.astype(jnp.bfloat16)).astype(jnp.float32)
        return accum_sum.astype(jnp.bfloat16).reshape(N_EP, CAP, D)
    results = lax.map(one_expert, (buffers, gate_stack, up_stack, down_stack))
    flat_results = results.reshape(experts * N_EP * CAP, D)
    row_index = ((route_flat * N_EP + blocks) * CAP + slot_of).astype(jnp.int32)
    gathered = flat_results[row_index].astype(jnp.float32)
    weights_flat = route_weights.reshape(N_EP, TOK_DEV, 2)
    gathered = gathered.reshape(N_EP, TOK_DEV, 2, D)
    combined = gathered[:, :, 0, :] * weights_flat[:, :, 0, None] + gathered[:, :, 1, :] * weights_flat[:, :, 1, None]
    combined = combined.reshape(N_EP * TOK_DEV, D)
    inv_second = lax.rsqrt(lax.optimization_barrier(jnp.mean(combined * combined, axis=1, keepdims=True)) + EPS)
    return (combined * inv_second * out_gain[None, :]).astype(jnp.bfloat16)
```

```python
import jax
import jax.numpy as jnp
from jax import lax
from jax.experimental import pallas as pl
from jax.experimental.pallas import tpu as pltpu
from jax.sharding import PartitionSpec as P

SPAN_EP = 2
EPS = 1e-06
MIB = 1 << 20


def front_body(home_ref, ids_ref, tok_ref, tgt_ref, *outs):
    experts = len(outs)
    capacity = outs[0].shape[0]
    tok_count = tok_ref.shape[0]
    home = home_ref[0]
    ids = ids_ref[...]
    pad = -(-experts // 8) * 8
    expert = lax.broadcasted_iota(jnp.int32, (pad, tok_count), 0)
    hot = [(ids[j : j + 1, :] == expert) for j in range(2)]
    either = (hot[0] | hot[1]).astype(jnp.float32).astype(jnp.bfloat16)
    earlier = (
        lax.broadcasted_iota(jnp.int32, (tok_count, tok_count), 0)
        < lax.broadcasted_iota(jnp.int32, (tok_count, tok_count), 1)
    ).astype(jnp.float32).astype(jnp.bfloat16)
    before = jnp.dot(either, earlier, preferred_element_type=jnp.float32)
    place = []
    for j in range(2):
        slot = jnp.sum(jnp.where(hot[j], before, 0.0), axis=0, keepdims=True).astype(jnp.int32)
        near = nearness(ids[j : j + 1, :], home, experts)
        place.append(near * capacity + slot)
        tgt_ref[j : j + 1, :] = place[j]
    tok = tok_ref[...]
    for k in range(experts):
        row = lax.broadcasted_iota(jnp.int32, (capacity, tok_count), 0) + k * capacity
        pick = ((place[0] == row) | (place[1] == row)).astype(jnp.float32).astype(jnp.bfloat16)
        outs[k][...] = jnp.dot(pick, tok, preferred_element_type=jnp.float32).astype(jnp.bfloat16)


def front(home, ids_t, tokens, experts, capacity):
    tok_count, width = tokens.shape
    vm = pl.BlockSpec(memory_space=pltpu.VMEM)
    return pl.pallas_call(
        front_body,
        out_shape=[jax.ShapeDtypeStruct((2, tok_count), jnp.int32)]
        + [jax.ShapeDtypeStruct((capacity, width), jnp.bfloat16)] * experts,
        in_specs=[pl.BlockSpec(memory_space=pltpu.SMEM), vm, vm],
        out_specs=[vm] * (experts + 1),
        compiler_params=pltpu.CompilerParams(vmem_limit_bytes=24 * MIB),
        name="front",
    )(home, ids_t, tokens)


def nearness(expert, home, experts):
    if experts & (experts - 1) == 0:
        return expert ^ home
    return lax.rem(expert - home + experts, experts)


def away(home, k, experts):
    if experts & (experts - 1) == 0:
        return home ^ k
    return (home + k) % experts


def cuts_of(units):
    first = -(-units // 256) * 128
    return ((0, first), (first, units - first)) if first < units else ((0, units),)


def ffn_body(side_ref, mine_ref, theirs_ref, gain_m, gain_t, wg, wu, wd, own, other,
             wg_v, wu_v, wd_v, x_v, h_v, sems):
    half = mine_ref.shape[1]
    units = wg_v.shape[1]
    side = side_ref[0]
    cuts = cuts_of(units)
    loads = []
    for c, (at, size) in enumerate(cuts):
        for w, v in ((wg, wg_v), (wu, wu_v)):
            loads.append((w.at[0, :, pl.ds(at, size)], v.at[:, pl.ds(at, size)]))
    for far in (1, 0):
        col = pl.multiple_of((side ^ far) * half, 128)
        loads.append((wd.at[0, :, pl.ds(col, half)], wd_v.at[far]))
    copies = [pltpu.make_async_copy(s, d, sems.at[n]) for n, (s, d) in enumerate(loads)]
    for copy in copies:
        copy.start()
    mine = mine_ref[...].astype(jnp.float32)
    theirs = theirs_ref[...].astype(jnp.float32)
    total = jnp.sum(mine * mine, axis=1, keepdims=True) + jnp.sum(theirs * theirs, axis=1, keepdims=True)
    scale = lax.rsqrt(total / (2 * half) + EPS)
    x_v[side] = (mine * scale * gain_m[...]).astype(jnp.bfloat16)
    x_v[1 - side] = (theirs * scale * gain_t[...]).astype(jnp.bfloat16)

    def product(w, at, size):
        return jnp.dot(
            x_v[0], w[0:half, at : at + size], preferred_element_type=jnp.float32
        ) + jnp.dot(x_v[1], w[half : 2 * half, at : at + size], preferred_element_type=jnp.float32)

    n = 0
    for at, size in cuts:
        copies[n].wait()
        gate = product(wg_v, at, size)
        copies[n + 1].wait()
        up = product(wu_v, at, size)
        n += 2
        h_v[:, at : at + size] = (gate / (1.0 + jnp.exp(-gate)) * up).astype(jnp.bfloat16)
    hidden = h_v[...]
    for far, out in ((1, other), (0, own)):
        copies[n].wait()
        n += 1
        out[...] = jnp.dot(hidden, wd_v[far], preferred_element_type=jnp.float32).astype(jnp.bfloat16)


def ffn(side, mine, theirs, gain_m, gain_t, w_gate, w_up, w_down):
    rows, half = mine.shape
    units = w_gate.shape[2]
    vm = pl.BlockSpec(memory_space=pltpu.VMEM)
    hbm = pl.BlockSpec(memory_space=pl.ANY)
    out = jax.ShapeDtypeStruct((rows, half), jnp.bfloat16)
    return pl.pallas_call(
        ffn_body,
        out_shape=[out, out],
        in_specs=[pl.BlockSpec(memory_space=pltpu.SMEM), vm, vm, vm, vm, hbm, hbm, hbm],
        out_specs=[vm, vm],
        scratch_shapes=[
            pltpu.VMEM((2 * half, units), jnp.bfloat16),
            pltpu.VMEM((2 * half, units), jnp.bfloat16),
            pltpu.VMEM((2, units, half), jnp.bfloat16),
            pltpu.VMEM((2, rows, half), jnp.bfloat16),
            pltpu.VMEM((rows, units), jnp.bfloat16),
            pltpu.SemaphoreType.DMA((2 * len(cuts_of(units)) + 2,)),
        ],
        compiler_params=pltpu.CompilerParams(vmem_limit_bytes=40 * MIB),
        cost_estimate=pl.CostEstimate(
            flops=12 * rows * half * units, transcendentals=rows * units, bytes_accessed=12 * half * units
        ),
        name="ffn",
    )(side, mine, theirs, gain_m, gain_t, w_gate, w_up, w_down)


def tail_body(tgt_ref, wts_ref, *refs):
    rows, out = refs[:-1], refs[-1]
    capacity = rows[0].shape[0]
    tok_count = tgt_ref.shape[1]
    total = None
    for j in range(2):
        picked = None
        for k, ref in enumerate(rows):
            row = lax.broadcasted_iota(jnp.int32, (capacity, tok_count), 0) + k * capacity
            pick = (tgt_ref[j : j + 1, :] == row).astype(jnp.float32).astype(jnp.bfloat16)
            part = lax.dot_general(
                pick, ref[...], (((0,), (0,)), ((), ())), preferred_element_type=jnp.float32
            )
            picked = part if picked is None else picked + part
        part = picked * wts_ref[:, j : j + 1]
        total = part if total is None else total + part
    out[...] = total


def tail(targets, weights, rows):
    tok_count = targets.shape[1]
    vm = pl.BlockSpec(memory_space=pltpu.VMEM)
    return pl.pallas_call(
        tail_body,
        out_shape=jax.ShapeDtypeStruct((tok_count, rows[0].shape[1]), jnp.float32),
        in_specs=[vm] * (2 + len(rows)),
        out_specs=vm,
        compiler_params=pltpu.CompilerParams(vmem_limit_bytes=24 * MIB),
        name="tail",
    )(targets, weights, *rows)


def per_device(tokens, in_gain, route_ids, route_weights, w_gate, w_up, w_down, out_gain):
    tok_count, half = tokens.shape
    ep_size = lax.axis_size("ep")
    tp_size = lax.axis_size("tp")
    experts = ep_size // SPAN_EP
    capacity = 2 * (5 * tok_count // (4 * experts))
    home = (lax.axis_index("ep") // SPAN_EP).astype(jnp.int32)
    side = lax.axis_index("tp").astype(jnp.int32).reshape(1)
    swap = [(i, i ^ 1) for i in range(tp_size)]

    def tp_swap(v):
        return lax.ppermute(v, "tp", swap)

    def member_swap(v):
        return lax.ppermute(v, "ep", [(i, i ^ 1) for i in range(ep_size)])

    def hop(v, k, back=False):
        if k == 0:
            return v
        pairs = [
            (e * SPAN_EP + i, away(e, k, experts) * SPAN_EP + i) for e in range(experts) for i in range(SPAN_EP)
        ]
        return lax.ppermute(v, "ep", [(b, a) for a, b in pairs] if back else pairs)

    gain_m = in_gain.reshape(1, half)
    gain_t = tp_swap(gain_m)
    targets, *rows = front(home.reshape(1), route_ids.T, tokens, experts, capacity)
    arrived = [hop(rows[k], k) for k in range(experts)]
    results = []
    for k in range(experts):
        mine = jnp.concatenate([arrived[k], member_swap(arrived[k])], axis=0)
        theirs = tp_swap(mine)
        own, other = ffn(side, mine, theirs, gain_m, gain_t, w_gate, w_up, w_down)
        pair = (own.astype(jnp.float32) + tp_swap(other).astype(jnp.float32)).astype(jnp.bfloat16)
        crossed = member_swap(pair[capacity:])
        result = (pair[:capacity].astype(jnp.float32) + crossed.astype(jnp.float32)).astype(jnp.bfloat16)
        results.append(hop(result, k, True))
    combined = tail(targets, route_weights, results)
    second_sum = lax.psum(jnp.sum(combined * combined, axis=1), "tp")
    return (combined * lax.rsqrt(second_sum[:, None] / (tp_size * half) + EPS) * out_gain[None, :]).astype(
        jnp.bfloat16
    )


def solution(mesh):
    placed = (
        P(("grp", "ep"), "tp"),
        P("tp"),
        P(("grp", "ep"), None),
        P(("grp", "ep"), None),
        P("ep", None, "tp"),
        P("ep", None, "tp"),
        P("ep", "tp", None),
        P("tp"),
    )
    return jax.shard_map(
        per_device, mesh=mesh, in_specs=placed, out_specs=P(("grp", "ep"), "tp"), check_vma=False
    )
```

```python
import jax
import jax.numpy as jnp
from jax import lax
from jax.experimental import pallas as pl
from jax.experimental.pallas import tpu as pltpu
from jax.sharding import PartitionSpec as P


SPAN_EP = 2
EPS = 1e-06
MIB = 1 << 20


def front_body(home_ref, ids_ref, tok_ref, tgt_ref, *outs):
    experts = len(outs)
    capacity = outs[0].shape[0]
    tok_count = tok_ref.shape[0]
    home = home_ref[0]
    ids = ids_ref[...]
    pad = -(-experts // 8) * 8
    expert = lax.broadcasted_iota(jnp.int32, (pad, tok_count), 0)
    hot = [(ids[j : j + 1, :] == expert) for j in range(2)]
    either = (hot[0] | hot[1]).astype(jnp.float32).astype(jnp.bfloat16)
    earlier = (
        lax.broadcasted_iota(jnp.int32, (tok_count, tok_count), 0)
        < lax.broadcasted_iota(jnp.int32, (tok_count, tok_count), 1)
    ).astype(jnp.float32).astype(jnp.bfloat16)
    before = jnp.dot(either, earlier, preferred_element_type=jnp.float32)
    place = []
    for j in range(2):
        slot = jnp.sum(jnp.where(hot[j], before, 0.0), axis=0, keepdims=True).astype(jnp.int32)
        near = nearness(ids[j : j + 1, :], home, experts)
        place.append(near * capacity + slot)
        tgt_ref[j : j + 1, :] = place[j]
    tok = tok_ref[...]
    for k in range(experts):
        row = lax.broadcasted_iota(jnp.int32, (capacity, tok_count), 0) + k * capacity
        pick = ((place[0] == row) | (place[1] == row)).astype(jnp.float32).astype(jnp.bfloat16)
        outs[k][...] = jnp.dot(pick, tok, preferred_element_type=jnp.float32).astype(jnp.bfloat16)


def front(home, ids_t, tokens, experts, capacity):
    tok_count, width = tokens.shape
    vm = pl.BlockSpec(memory_space=pltpu.VMEM)
    return pl.pallas_call(
        front_body,
        out_shape=[jax.ShapeDtypeStruct((2, tok_count), jnp.int32)]
        + [jax.ShapeDtypeStruct((capacity, width), jnp.bfloat16)] * experts,
        in_specs=[pl.BlockSpec(memory_space=pltpu.SMEM), vm, vm],
        out_specs=[vm] * (experts + 1),
        compiler_params=pltpu.CompilerParams(vmem_limit_bytes=12 * MIB),
        name="front",
    )(home, ids_t, tokens)


def nearness(expert, home, experts):
    if experts & (experts - 1) == 0:
        return expert ^ home
    return lax.rem(expert - home + experts, experts)


def away(home, k, experts):
    if experts & (experts - 1) == 0:
        return home ^ k
    return (home + k) % experts


def cuts_of(units):
    first = -(-units // 256) * 128
    return ((0, first), (first, units - first)) if first < units else ((0, units),)


def ffn_body(side_ref, mine_ref, theirs_ref, gain_m, gain_t, wg, wu, wd, own, other,
             wg_v, wu_v, wd_v, x_v, h_v, sems):
    half = mine_ref.shape[1]
    units = wg_v.shape[1]
    side = side_ref[0]
    cuts = cuts_of(units)
    loads = []
    for at, size in cuts:
        for w, v in ((wg, wg_v), (wu, wu_v)):
            loads.append((w.at[0, :, pl.ds(at, size)], v.at[:, pl.ds(at, size)]))
    for far in (1, 0):
        col = pl.multiple_of((side ^ far) * half, 128)
        loads.append((wd.at[0, :, pl.ds(col, half)], wd_v.at[far]))
    copies = [pltpu.make_async_copy(s, d, sems.at[n]) for n, (s, d) in enumerate(loads)]
    for copy in copies:
        copy.start()
    mine = mine_ref[...].astype(jnp.float32)
    theirs = theirs_ref[...].astype(jnp.float32)
    total = jnp.sum(mine * mine, axis=1, keepdims=True) + jnp.sum(theirs * theirs, axis=1, keepdims=True)
    scale = lax.rsqrt(total / (2 * half) + EPS)
    x_v[side] = (mine * scale * gain_m[...]).astype(jnp.bfloat16)
    x_v[1 - side] = (theirs * scale * gain_t[...]).astype(jnp.bfloat16)

    def product(w, at, size):
        return jnp.dot(
            x_v[0], w[0:half, at : at + size], preferred_element_type=jnp.float32
        ) + jnp.dot(x_v[1], w[half : 2 * half, at : at + size], preferred_element_type=jnp.float32)

    n = 0
    for at, size in cuts:
        copies[n].wait()
        gate = product(wg_v, at, size)
        copies[n + 1].wait()
        up = product(wu_v, at, size)
        n += 2
        h_v[:, at : at + size] = (gate / (1.0 + jnp.exp(-gate)) * up).astype(jnp.bfloat16)
    hidden = h_v[...]
    for far, out in ((1, other), (0, own)):
        copies[n].wait()
        n += 1
        out[...] = jnp.dot(hidden, wd_v[far], preferred_element_type=jnp.float32).astype(jnp.bfloat16)


def ffn(side, mine, theirs, gain_m, gain_t, w_gate, w_up, w_down):
    rows, half = mine.shape
    units = w_gate.shape[2]
    vm = pl.BlockSpec(memory_space=pltpu.VMEM)
    hbm = pl.BlockSpec(memory_space=pl.ANY)
    out = jax.ShapeDtypeStruct((rows, half), jnp.bfloat16)
    return pl.pallas_call(
        ffn_body,
        out_shape=[out, out],
        in_specs=[pl.BlockSpec(memory_space=pltpu.SMEM), vm, vm, vm, vm, hbm, hbm, hbm],
        out_specs=[vm, vm],
        scratch_shapes=[
            pltpu.VMEM((2 * half, units), jnp.bfloat16),
            pltpu.VMEM((2 * half, units), jnp.bfloat16),
            pltpu.VMEM((2, units, half), jnp.bfloat16),
            pltpu.VMEM((2, rows, half), jnp.bfloat16),
            pltpu.VMEM((rows, units), jnp.bfloat16),
            pltpu.SemaphoreType.DMA((2 * len(cuts_of(units)) + 2,)),
        ],
        compiler_params=pltpu.CompilerParams(vmem_limit_bytes=49 * MIB),
        cost_estimate=pl.CostEstimate(
            flops=12 * rows * half * units, transcendentals=rows * units, bytes_accessed=12 * half * units
        ),
        name="ffn",
    )(side, mine, theirs, gain_m, gain_t, w_gate, w_up, w_down)


def tail_body(tgt_ref, wts_ref, *refs):
    rows, out = refs[:-1], refs[-1]
    capacity = rows[0].shape[0]
    tok_count = tgt_ref.shape[1]
    total = None
    for j in range(2):
        picked = None
        for k, ref in enumerate(rows):
            row = lax.broadcasted_iota(jnp.int32, (capacity, tok_count), 0) + k * capacity
            pick = (tgt_ref[j : j + 1, :] == row).astype(jnp.float32).astype(jnp.bfloat16)
            part = lax.dot_general(
                pick, ref[...], (((0,), (0,)), ((), ())), preferred_element_type=jnp.float32
            )
            picked = part if picked is None else picked + part
        part = picked * wts_ref[:, j : j + 1]
        total = part if total is None else total + part
    out[...] = total


def tail(targets, weights, rows):
    tok_count = targets.shape[1]
    vm = pl.BlockSpec(memory_space=pltpu.VMEM)
    return pl.pallas_call(
        tail_body,
        out_shape=jax.ShapeDtypeStruct((tok_count, rows[0].shape[1]), jnp.float32),
        in_specs=[vm] * (2 + len(rows)),
        out_specs=vm,
        compiler_params=pltpu.CompilerParams(vmem_limit_bytes=12 * MIB),
        name="tail",
    )(targets, weights, *rows)


def per_device(tokens, in_gain, route_ids, route_weights, w_gate, w_up, w_down, out_gain):
    tok_count, half = tokens.shape
    ep_size = lax.axis_size("ep")
    tp_size = lax.axis_size("tp")
    experts = ep_size // SPAN_EP
    capacity = 2 * (5 * tok_count // (4 * experts))
    home = (lax.axis_index("ep") // SPAN_EP).astype(jnp.int32)
    side = lax.axis_index("tp").astype(jnp.int32).reshape(1)
    swap = [(i, i ^ 1) for i in range(tp_size)]

    def tp_swap(v):
        return lax.ppermute(v, "tp", swap)

    def member_swap(v):
        return lax.ppermute(v, "ep", [(i, i ^ 1) for i in range(ep_size)])

    def hop(v, k, back=False):
        if k == 0:
            return v
        pairs = [
            (e * SPAN_EP + i, away(e, k, experts) * SPAN_EP + i) for e in range(experts) for i in range(SPAN_EP)
        ]
        return lax.ppermute(v, "ep", [(b, a) for a, b in pairs] if back else pairs)

    gain_m = in_gain.reshape(1, half)
    gain_t = tp_swap(gain_m)
    targets, *rows = front(home.reshape(1), route_ids.T, tokens, experts, capacity)
    results = []
    for k in range(experts):
        near = hop(rows[k], k)
        crossed = member_swap(near)
        mine = jnp.concatenate([near, crossed], axis=0)
        theirs = tp_swap(mine)
        own, other = ffn(side, mine, theirs, gain_m, gain_t, w_gate, w_up, w_down)
        back = tp_swap(other)
        pair = (own.astype(jnp.float32) + back.astype(jnp.float32)).astype(jnp.bfloat16)
        crossed = member_swap(pair[capacity:])
        result = (pair[:capacity].astype(jnp.float32) + crossed.astype(jnp.float32)).astype(jnp.bfloat16)
        results.append(hop(result, k, True))
    combined = tail(targets, route_weights, results)
    second_sum = lax.psum(jnp.sum(combined * combined, axis=1), "tp")
    return (combined * lax.rsqrt(second_sum[:, None] / (tp_size * half) + EPS) * out_gain[None, :]).astype(jnp.bfloat16)


def solution(mesh):
    placed = (
        P(("grp", "ep"), "tp"),
        P("tp"),
        P(("grp", "ep"), None),
        P(("grp", "ep"), None),
        P("ep", None, "tp"),
        P("ep", None, "tp"),
        P("ep", "tp", None),
        P("tp"),
    )
    return jax.shard_map(
        per_device, mesh=mesh, in_specs=placed, out_specs=P(("grp", "ep"), "tp"), check_vma=False
    )
```

```python
import jax
import jax.numpy as jnp
from jax import lax
from jax.experimental import pallas as pl
from jax.experimental.pallas import tpu as pltpu
from jax.sharding import PartitionSpec as P


SPAN_EP = 2
EPS = 1e-06
MIB = 1 << 20


def front_body(home_ref, ids_ref, tok_ref, tgt_ref, *outs):
    experts = len(outs)
    capacity = outs[0].shape[0]
    tok_count = tok_ref.shape[0]
    home = home_ref[0]
    ids = ids_ref[...]
    pad = -(-experts // 8) * 8
    expert = lax.broadcasted_iota(jnp.int32, (pad, tok_count), 0)
    hot = [(ids[j : j + 1, :] == expert) for j in range(2)]
    either = (hot[0] | hot[1]).astype(jnp.float32).astype(jnp.bfloat16)
    earlier = (
        lax.broadcasted_iota(jnp.int32, (tok_count, tok_count), 0)
        < lax.broadcasted_iota(jnp.int32, (tok_count, tok_count), 1)
    ).astype(jnp.float32).astype(jnp.bfloat16)
    before = jnp.dot(either, earlier, preferred_element_type=jnp.float32)
    place = []
    for j in range(2):
        slot = jnp.sum(jnp.where(hot[j], before, 0.0), axis=0, keepdims=True).astype(jnp.int32)
        near = nearness(ids[j : j + 1, :], home, experts)
        place.append(near * capacity + slot)
        tgt_ref[j : j + 1, :] = place[j]
    tok = tok_ref[...]
    for k in range(experts):
        row = lax.broadcasted_iota(jnp.int32, (capacity, tok_count), 0) + k * capacity
        pick = ((place[0] == row) | (place[1] == row)).astype(jnp.float32).astype(jnp.bfloat16)
        outs[k][...] = jnp.dot(pick, tok, preferred_element_type=jnp.float32).astype(jnp.bfloat16)


def front(home, ids_t, tokens, experts, capacity):
    tok_count, width = tokens.shape
    vm = pl.BlockSpec(memory_space=pltpu.VMEM)
    return pl.pallas_call(
        front_body,
        out_shape=[jax.ShapeDtypeStruct((2, tok_count), jnp.int32)]
        + [jax.ShapeDtypeStruct((capacity, width), jnp.bfloat16)] * experts,
        in_specs=[pl.BlockSpec(memory_space=pltpu.SMEM), vm, vm],
        out_specs=[vm] * (experts + 1),
        compiler_params=pltpu.CompilerParams(vmem_limit_bytes=12 * MIB),
        name="front",
    )(home, ids_t, tokens)


def nearness(expert, home, experts):
    if experts & (experts - 1) == 0:
        return expert ^ home
    return lax.rem(expert - home + experts, experts)


def pieces(v, apart):
    if not apart:
        return [v]
    middle = v.shape[0] * 2 // 5 // 16 * 16
    return [v[:middle], v[middle:]]


def away(home, k, experts):
    if experts & (experts - 1) == 0:
        return home ^ k
    return (home + k) % experts


def cuts_of(units):
    first = -(-units // 256) * 128
    return ((0, first), (first, units - first)) if first < units else ((0, units),)


def ffn_body(side_ref, mine_ref, theirs_ref, gain_m, gain_t, wg, wu, wd, own, other,
             wg_v, wu_v, wd_v, x_v, h_v, sems):
    half = mine_ref.shape[1]
    units = wg_v.shape[1]
    side = side_ref[0]
    cuts = cuts_of(units)
    loads = []
    for at, size in cuts:
        for w, v in ((wg, wg_v), (wu, wu_v)):
            loads.append((w.at[0, :, pl.ds(at, size)], v.at[:, pl.ds(at, size)]))
    for far in (1, 0):
        col = pl.multiple_of((side ^ far) * half, 128)
        loads.append((wd.at[0, :, pl.ds(col, half)], wd_v.at[far]))
    copies = [pltpu.make_async_copy(s, d, sems.at[n]) for n, (s, d) in enumerate(loads)]
    for copy in copies:
        copy.start()
    mine = mine_ref[...].astype(jnp.float32)
    theirs = theirs_ref[...].astype(jnp.float32)
    total = jnp.sum(mine * mine, axis=1, keepdims=True) + jnp.sum(theirs * theirs, axis=1, keepdims=True)
    scale = lax.rsqrt(total / (2 * half) + EPS)
    x_v[side] = (mine * scale * gain_m[...]).astype(jnp.bfloat16)
    x_v[1 - side] = (theirs * scale * gain_t[...]).astype(jnp.bfloat16)

    def product(w, at, size):
        return jnp.dot(
            x_v[0], w[0:half, at : at + size], preferred_element_type=jnp.float32
        ) + jnp.dot(x_v[1], w[half : 2 * half, at : at + size], preferred_element_type=jnp.float32)

    n = 0
    for at, size in cuts:
        copies[n].wait()
        gate = product(wg_v, at, size)
        copies[n + 1].wait()
        up = product(wu_v, at, size)
        n += 2
        h_v[:, at : at + size] = (gate / (1.0 + jnp.exp(-gate)) * up).astype(jnp.bfloat16)
    hidden = h_v[...]
    for far, out in ((1, other), (0, own)):
        copies[n].wait()
        n += 1
        out[...] = jnp.dot(hidden, wd_v[far], preferred_element_type=jnp.float32).astype(jnp.bfloat16)


def ffn(side, mine, theirs, gain_m, gain_t, w_gate, w_up, w_down):
    rows, half = mine.shape
    units = w_gate.shape[2]
    vm = pl.BlockSpec(memory_space=pltpu.VMEM)
    hbm = pl.BlockSpec(memory_space=pl.ANY)
    out = jax.ShapeDtypeStruct((rows, half), jnp.bfloat16)
    return pl.pallas_call(
        ffn_body,
        out_shape=[out, out],
        in_specs=[pl.BlockSpec(memory_space=pltpu.SMEM), vm, vm, vm, vm, hbm, hbm, hbm],
        out_specs=[vm, vm],
        scratch_shapes=[
            pltpu.VMEM((2 * half, units), jnp.bfloat16),
            pltpu.VMEM((2 * half, units), jnp.bfloat16),
            pltpu.VMEM((2, units, half), jnp.bfloat16),
            pltpu.VMEM((2, rows, half), jnp.bfloat16),
            pltpu.VMEM((rows, units), jnp.bfloat16),
            pltpu.SemaphoreType.DMA((2 * len(cuts_of(units)) + 2,)),
        ],
        compiler_params=pltpu.CompilerParams(vmem_limit_bytes=49 * MIB),
        cost_estimate=pl.CostEstimate(
            flops=12 * rows * half * units, transcendentals=rows * units, bytes_accessed=12 * half * units
        ),
        name="ffn",
    )(side, mine, theirs, gain_m, gain_t, w_gate, w_up, w_down)


def resident_body(side_ref, mine_ref, theirs_ref, gain_m, gain_t, wg, wu, wd, own, other, x_v, h_v):
    half = mine_ref.shape[1]
    units = wg.shape[2]
    side = side_ref[0]
    mine = mine_ref[...].astype(jnp.float32)
    theirs = theirs_ref[...].astype(jnp.float32)
    total = jnp.sum(mine * mine, axis=1, keepdims=True) + jnp.sum(theirs * theirs, axis=1, keepdims=True)
    scale = lax.rsqrt(total / (2 * half) + EPS)
    x_v[side] = (mine * scale * gain_m[...]).astype(jnp.bfloat16)
    x_v[1 - side] = (theirs * scale * gain_t[...]).astype(jnp.bfloat16)

    def product(w, at, size):
        return jnp.dot(
            x_v[0], w[0, 0:half, at : at + size], preferred_element_type=jnp.float32
        ) + jnp.dot(x_v[1], w[0, half : 2 * half, at : at + size], preferred_element_type=jnp.float32)

    for at, size in cuts_of(units):
        gate = product(wg, at, size)
        up = product(wu, at, size)
        h_v[:, at : at + size] = (gate / (1.0 + jnp.exp(-gate)) * up).astype(jnp.bfloat16)
    hidden = h_v[...]
    for far, out in ((1, other), (0, own)):
        col = pl.multiple_of((side ^ far) * half, 128)
        out[...] = jnp.dot(
            hidden, wd[0, :, pl.ds(col, half)], preferred_element_type=jnp.float32
        ).astype(jnp.bfloat16)


def resident_ffn(side, mine, theirs, gain_m, gain_t, w_gate, w_up, w_down):
    rows, half = mine.shape
    units = w_gate.shape[2]
    vm = pl.BlockSpec(memory_space=pltpu.VMEM)
    out = jax.ShapeDtypeStruct((rows, half), jnp.bfloat16)
    return pl.pallas_call(
        resident_body,
        out_shape=[out, out],
        in_specs=[pl.BlockSpec(memory_space=pltpu.SMEM)] + [vm] * 7,
        out_specs=[vm, vm],
        scratch_shapes=[
            pltpu.VMEM((2, rows, half), jnp.bfloat16),
            pltpu.VMEM((rows, units), jnp.bfloat16),
        ],
        compiler_params=pltpu.CompilerParams(vmem_limit_bytes=16 * MIB),
        cost_estimate=pl.CostEstimate(
            flops=12 * rows * half * units, transcendentals=rows * units, bytes_accessed=12 * half * units
        ),
        name="ffn",
    )(side, mine, theirs, gain_m, gain_t, w_gate, w_up, w_down)


def keep_body(wg, wu, wd, *refs):
    refs[-1][...] = refs[0][...]


def keep(value, *weights):
    vm = pl.BlockSpec(memory_space=pltpu.VMEM)
    return pl.pallas_call(
        keep_body,
        out_shape=jax.ShapeDtypeStruct(value.shape, value.dtype),
        in_specs=[vm] * 4,
        out_specs=vm,
        compiler_params=pltpu.CompilerParams(vmem_limit_bytes=16 * MIB),
        name="keep",
    )(*weights, value)


def tail_body(tgt_ref, wts_ref, *refs):
    rows, out = refs[:-1], refs[-1]
    tok_count = tgt_ref.shape[1]
    total = None
    for j in range(2):
        picked, at = None, 0
        for ref in rows:
            size = ref.shape[0]
            row = lax.broadcasted_iota(jnp.int32, (size, tok_count), 0) + at
            at += size
            pick = (tgt_ref[j : j + 1, :] == row).astype(jnp.float32).astype(jnp.bfloat16)
            part = lax.dot_general(
                pick, ref[...], (((0,), (0,)), ((), ())), preferred_element_type=jnp.float32
            )
            picked = part if picked is None else picked + part
        part = picked * wts_ref[:, j : j + 1]
        total = part if total is None else total + part
    out[...] = total


def tail(targets, weights, rows):
    tok_count = targets.shape[1]
    vm = pl.BlockSpec(memory_space=pltpu.VMEM)
    return pl.pallas_call(
        tail_body,
        out_shape=jax.ShapeDtypeStruct((tok_count, rows[0].shape[1]), jnp.float32),
        in_specs=[vm] * (2 + len(rows)),
        out_specs=vm,
        compiler_params=pltpu.CompilerParams(vmem_limit_bytes=12 * MIB),
        name="tail",
    )(targets, weights, *rows)


def per_device(tokens, in_gain, route_ids, route_weights, w_gate, w_up, w_down, out_gain):
    tok_count, half = tokens.shape
    ep_size = lax.axis_size("ep")
    tp_size = lax.axis_size("tp")
    experts = ep_size // SPAN_EP
    capacity = 2 * (5 * tok_count // (4 * experts))
    home = (lax.axis_index("ep") // SPAN_EP).astype(jnp.int32)
    side = lax.axis_index("tp").astype(jnp.int32).reshape(1)
    swap = [(i, i ^ 1) for i in range(tp_size)]

    def tp_swap(v):
        return lax.ppermute(v, "tp", swap)

    def member_swap(v):
        return lax.ppermute(v, "ep", [(i, i ^ 1) for i in range(ep_size)])

    def hop(v, k, back=False):
        if k == 0:
            return v
        pairs = [
            (e * SPAN_EP + i, away(e, k, experts) * SPAN_EP + i) for e in range(experts) for i in range(SPAN_EP)
        ]
        return lax.ppermute(v, "ep", [(b, a) for a, b in pairs] if back else pairs)

    gain_m = in_gain.reshape(1, half)
    gain_t = tp_swap(gain_m)
    targets, *rows = front(home.reshape(1), route_ids.T, tokens, experts, capacity)
    weights = (w_gate, w_up, w_down)
    apart = capacity % 32 == 0
    gain_m = keep(gain_m, *weights)
    results = []
    for k in range(experts):
        far = apart and 2 * k >= experts
        near = []
        for piece in pieces(rows[k], far and 2 * k == experts):
            near.append(hop(piece, k))
        crossed = []
        for piece in near:
            crossed.append(member_swap(piece))
        mine = jnp.concatenate(near + crossed, axis=0)
        theirs = tp_swap(mine)
        if k == 1:
            gain_m = keep(gain_m, *weights)
        own, other = (resident_ffn if k else ffn)(side, mine, theirs, gain_m, gain_t, *weights)
        back = tp_swap(other)
        pair = (own.astype(jnp.float32) + back.astype(jnp.float32)).astype(jnp.bfloat16)
        kept = pieces(pair[:capacity], far)
        for p, piece in enumerate(pieces(pair[capacity:], far)):
            cross = member_swap(piece)
            result = (kept[p].astype(jnp.float32) + cross.astype(jnp.float32)).astype(jnp.bfloat16)
            results.append(hop(result, k, True))
    combined = tail(targets, route_weights, results)
    second_sum = lax.psum(jnp.sum(combined * combined, axis=1), "tp")
    return (combined * lax.rsqrt(second_sum[:, None] / (tp_size * half) + EPS) * out_gain[None, :]).astype(jnp.bfloat16)


def solution(mesh):
    placed = (
        P(("grp", "ep"), "tp"),
        P("tp"),
        P(("grp", "ep"), None),
        P(("grp", "ep"), None),
        P("ep", None, "tp"),
        P("ep", None, "tp"),
        P("ep", "tp", None),
        P("tp"),
    )
    return jax.shard_map(
        per_device, mesh=mesh, in_specs=placed, out_specs=P(("grp", "ep"), "tp"), check_vma=False
    )
```

```python
import functools

import jax
import jax.numpy as jnp
from jax import lax
from jax.experimental import pallas as pl
from jax.experimental.pallas import tpu as pltpu
from jax.sharding import PartitionSpec as P


SPAN_EP = 2
EPS = 1e-06
MIB = 1 << 20


def front_body(home_ref, ids_ref, tok_ref, tgt_ref, *outs, experts, capacity):
    tok_count = tok_ref.shape[0]
    home = home_ref[0]
    ids = ids_ref[...]
    pad = -(-experts // 8) * 8
    expert = lax.broadcasted_iota(jnp.int32, (pad, tok_count), 0)
    hot = [(ids[j : j + 1, :] == expert) for j in range(2)]
    either = (hot[0] | hot[1]).astype(jnp.float32).astype(jnp.bfloat16)
    earlier = (
        lax.broadcasted_iota(jnp.int32, (tok_count, tok_count), 0)
        < lax.broadcasted_iota(jnp.int32, (tok_count, tok_count), 1)
    ).astype(jnp.float32).astype(jnp.bfloat16)
    before = jnp.dot(either, earlier, preferred_element_type=jnp.float32)
    place = []
    for j in range(2):
        slot = jnp.sum(jnp.where(hot[j], before, 0.0), axis=0, keepdims=True).astype(jnp.int32)
        near = nearness(ids[j : j + 1, :], home, experts)
        place.append(near * capacity + slot)
        tgt_ref[j : j + 1, :] = place[j]
    tok = tok_ref[...]
    at = 0
    for out in outs:
        row = lax.broadcasted_iota(jnp.int32, (out.shape[0], tok_count), 0) + at
        at += out.shape[0]
        pick = ((place[0] == row) | (place[1] == row)).astype(jnp.float32).astype(jnp.bfloat16)
        out[...] = jnp.dot(pick, tok, preferred_element_type=jnp.float32).astype(jnp.bfloat16)


def front(home, ids_t, tokens, experts, capacity, sizes):
    tok_count, width = tokens.shape
    vm = pl.BlockSpec(memory_space=pltpu.VMEM)
    return pl.pallas_call(
        functools.partial(front_body, experts=experts, capacity=capacity),
        out_shape=[jax.ShapeDtypeStruct((2, tok_count), jnp.int32)]
        + [jax.ShapeDtypeStruct((size, width), jnp.bfloat16) for size in sizes],
        in_specs=[pl.BlockSpec(memory_space=pltpu.SMEM), vm, vm],
        out_specs=[vm] * (len(sizes) + 1),
        compiler_params=pltpu.CompilerParams(vmem_limit_bytes=12 * MIB),
        name="front",
    )(home, ids_t, tokens)


def nearness(expert, home, experts):
    if experts & (experts - 1) == 0:
        return expert ^ home
    return lax.rem(expert - home + experts, experts)


def sizes_of(capacity, apart):
    first = capacity * 2 // 5 // 16 * 16
    return (first, capacity - first) if apart and first else (capacity,)


def pieces(v, sizes):
    out, at = [], 0
    for size in sizes:
        out.append(v[at : at + size])
        at += size
    return out


def away(home, k, experts):
    if experts & (experts - 1) == 0:
        return home ^ k
    return (home + k) % experts


def cuts_of(units):
    first = -(-units // 256) * 128
    return ((0, first), (first, units - first)) if first < units else ((0, units),)


def ffn_body(side_ref, mine_ref, theirs_ref, gain_m, gain_t, wg, wu, wd, own, other,
             wg_v, wu_v, wd_v, x_v, h_v, sems):
    half = mine_ref.shape[1]
    units = wg_v.shape[1]
    side = side_ref[0]
    cuts = cuts_of(units)
    loads = []
    for at, size in cuts:
        for w, v in ((wg, wg_v), (wu, wu_v)):
            loads.append((w.at[0, :, pl.ds(at, size)], v.at[:, pl.ds(at, size)]))
    for far in (1, 0):
        col = pl.multiple_of((side ^ far) * half, 128)
        loads.append((wd.at[0, :, pl.ds(col, half)], wd_v.at[far]))
    copies = [pltpu.make_async_copy(s, d, sems.at[n]) for n, (s, d) in enumerate(loads)]
    for copy in copies:
        copy.start()
    mine = mine_ref[...].astype(jnp.float32)
    theirs = theirs_ref[...].astype(jnp.float32)
    total = jnp.sum(mine * mine, axis=1, keepdims=True) + jnp.sum(theirs * theirs, axis=1, keepdims=True)
    scale = lax.rsqrt(total / (2 * half) + EPS)
    x_v[side] = (mine * scale * gain_m[...]).astype(jnp.bfloat16)
    x_v[1 - side] = (theirs * scale * gain_t[...]).astype(jnp.bfloat16)

    def product(w, at, size):
        return jnp.dot(
            x_v[0], w[0:half, at : at + size], preferred_element_type=jnp.float32
        ) + jnp.dot(x_v[1], w[half : 2 * half, at : at + size], preferred_element_type=jnp.float32)

    n = 0
    for at, size in cuts:
        copies[n].wait()
        gate = product(wg_v, at, size)
        copies[n + 1].wait()
        up = product(wu_v, at, size)
        n += 2
        h_v[:, at : at + size] = (gate / (1.0 + jnp.exp(-gate)) * up).astype(jnp.bfloat16)
    hidden = h_v[...]
    for far, out in ((1, other), (0, own)):
        copies[n].wait()
        n += 1
        out[...] = jnp.dot(hidden, wd_v[far], preferred_element_type=jnp.float32).astype(jnp.bfloat16)


def ffn(side, mine, theirs, gain_m, gain_t, w_gate, w_up, w_down):
    rows, half = mine.shape
    units = w_gate.shape[2]
    vm = pl.BlockSpec(memory_space=pltpu.VMEM)
    hbm = pl.BlockSpec(memory_space=pl.ANY)
    out = jax.ShapeDtypeStruct((rows, half), jnp.bfloat16)
    return pl.pallas_call(
        ffn_body,
        out_shape=[out, out],
        in_specs=[pl.BlockSpec(memory_space=pltpu.SMEM), vm, vm, vm, vm, hbm, hbm, hbm],
        out_specs=[vm, vm],
        scratch_shapes=[
            pltpu.VMEM((2 * half, units), jnp.bfloat16),
            pltpu.VMEM((2 * half, units), jnp.bfloat16),
            pltpu.VMEM((2, units, half), jnp.bfloat16),
            pltpu.VMEM((2, rows, half), jnp.bfloat16),
            pltpu.VMEM((rows, units), jnp.bfloat16),
            pltpu.SemaphoreType.DMA((2 * len(cuts_of(units)) + 2,)),
        ],
        compiler_params=pltpu.CompilerParams(vmem_limit_bytes=51 * MIB),
        cost_estimate=pl.CostEstimate(
            flops=12 * rows * half * units, transcendentals=rows * units, bytes_accessed=12 * half * units
        ),
        name="ffn",
    )(side, mine, theirs, gain_m, gain_t, w_gate, w_up, w_down)


def resident_body(side_ref, mine_ref, theirs_ref, gain_m, gain_t, wg, wu, wd, own, other, x_v, h_v):
    half = mine_ref.shape[1]
    units = wg.shape[2]
    side = side_ref[0]
    mine = mine_ref[...].astype(jnp.float32)
    theirs = theirs_ref[...].astype(jnp.float32)
    total = jnp.sum(mine * mine, axis=1, keepdims=True) + jnp.sum(theirs * theirs, axis=1, keepdims=True)
    scale = lax.rsqrt(total / (2 * half) + EPS)
    x_v[side] = (mine * scale * gain_m[...]).astype(jnp.bfloat16)
    x_v[1 - side] = (theirs * scale * gain_t[...]).astype(jnp.bfloat16)

    def product(w, at, size):
        return jnp.dot(
            x_v[0], w[0, 0:half, at : at + size], preferred_element_type=jnp.float32
        ) + jnp.dot(x_v[1], w[0, half : 2 * half, at : at + size], preferred_element_type=jnp.float32)

    for at, size in cuts_of(units):
        gate = product(wg, at, size)
        up = product(wu, at, size)
        h_v[:, at : at + size] = (gate / (1.0 + jnp.exp(-gate)) * up).astype(jnp.bfloat16)
    hidden = h_v[...]
    for far, out in ((1, other), (0, own)):
        col = pl.multiple_of((side ^ far) * half, 128)
        out[...] = jnp.dot(
            hidden, wd[0, :, pl.ds(col, half)], preferred_element_type=jnp.float32
        ).astype(jnp.bfloat16)


def resident_ffn(side, mine, theirs, gain_m, gain_t, w_gate, w_up, w_down):
    rows, half = mine.shape
    units = w_gate.shape[2]
    vm = pl.BlockSpec(memory_space=pltpu.VMEM)
    out = jax.ShapeDtypeStruct((rows, half), jnp.bfloat16)
    return pl.pallas_call(
        resident_body,
        out_shape=[out, out],
        in_specs=[pl.BlockSpec(memory_space=pltpu.SMEM)] + [vm] * 7,
        out_specs=[vm, vm],
        scratch_shapes=[
            pltpu.VMEM((2, rows, half), jnp.bfloat16),
            pltpu.VMEM((rows, units), jnp.bfloat16),
        ],
        compiler_params=pltpu.CompilerParams(vmem_limit_bytes=16 * MIB),
        cost_estimate=pl.CostEstimate(
            flops=12 * rows * half * units, transcendentals=rows * units, bytes_accessed=12 * half * units
        ),
        name="ffn",
    )(side, mine, theirs, gain_m, gain_t, w_gate, w_up, w_down)


def keep_body(wg, wu, wd, *refs):
    refs[-1][...] = refs[0][...]


def keep(value, *weights):
    vm = pl.BlockSpec(memory_space=pltpu.VMEM)
    return pl.pallas_call(
        keep_body,
        out_shape=jax.ShapeDtypeStruct(value.shape, value.dtype),
        in_specs=[vm] * 4,
        out_specs=vm,
        compiler_params=pltpu.CompilerParams(vmem_limit_bytes=16 * MIB),
        name="keep",
    )(*weights, value)


def tail_body(tgt_ref, wts_ref, *refs, places):
    rows, out = refs[: len(places)], refs[-1]
    tok_count = tgt_ref.shape[1]
    total = refs[len(places)][...] if len(refs) > len(places) + 1 else None
    for j in range(2):
        picked = None
        for at, ref in zip(places, rows):
            row = lax.broadcasted_iota(jnp.int32, (ref.shape[0], tok_count), 0) + at
            pick = (tgt_ref[j : j + 1, :] == row).astype(jnp.float32).astype(jnp.bfloat16)
            part = lax.dot_general(
                pick, ref[...], (((0,), (0,)), ((), ())), preferred_element_type=jnp.float32
            )
            picked = part if picked is None else picked + part
        part = picked * wts_ref[:, j : j + 1]
        total = part if total is None else total + part
    out[...] = total


def tail(targets, weights, rows, *total):
    tok_count = targets.shape[1]
    vm = pl.BlockSpec(memory_space=pltpu.VMEM)
    return pl.pallas_call(
        functools.partial(tail_body, places=tuple(at for at, _ in rows)),
        out_shape=jax.ShapeDtypeStruct((tok_count, rows[0][1].shape[1]), jnp.float32),
        in_specs=[vm] * (2 + len(rows) + len(total)),
        out_specs=vm,
        compiler_params=pltpu.CompilerParams(vmem_limit_bytes=12 * MIB),
        name="tail",
    )(targets, weights, *[r for _, r in rows], *total)


def per_device(tokens, in_gain, route_ids, route_weights, w_gate, w_up, w_down, out_gain):
    tok_count, half = tokens.shape
    ep_size = lax.axis_size("ep")
    tp_size = lax.axis_size("tp")
    experts = ep_size // SPAN_EP
    capacity = 2 * (5 * tok_count // (4 * experts))
    home = (lax.axis_index("ep") // SPAN_EP).astype(jnp.int32)
    side = lax.axis_index("tp").astype(jnp.int32).reshape(1)
    swap = [(i, i ^ 1) for i in range(tp_size)]

    def tp_swap(v):
        return lax.ppermute(v, "tp", swap)

    def member_swap(v):
        return lax.ppermute(v, "ep", [(i, i ^ 1) for i in range(ep_size)])

    def hop(v, k, back=False):
        if k == 0:
            return v
        pairs = [
            (e * SPAN_EP + i, away(e, k, experts) * SPAN_EP + i) for e in range(experts) for i in range(SPAN_EP)
        ]
        return lax.ppermute(v, "ep", [(b, a) for a, b in pairs] if back else pairs)

    gain_m = in_gain.reshape(1, half)
    apart = capacity % 32 == 0
    gain_t = tp_swap(gain_m)
    cut_in = [sizes_of(capacity, apart and 2 * k == experts) for k in range(experts)]
    cut_back = [sizes_of(capacity, apart and 2 * k >= experts) for k in range(experts)]
    flat = [size for sizes in cut_in for size in sizes]
    targets, *sent = front(home.reshape(1), route_ids.T, tokens, experts, capacity, flat)
    weights = (w_gate, w_up, w_down)
    stream = (0, experts // 2)
    gain_r = gain_m
    gain_r = keep(gain_m, *weights)
    results = []
    for k in range(experts):
        near = []
        for _ in range(len(cut_in[k])):
            piece = sent.pop(0)
            near.append(hop(piece, k))
        crossed = []
        for piece in near:
            crossed.append(member_swap(piece))
        mine = jnp.concatenate(near + crossed, axis=0)
        theirs = tp_swap(mine)
        if k in stream:
            own, other = ffn(side, mine, theirs, gain_m, gain_t, *weights)
        else:
            own, other = resident_ffn(side, mine, theirs, gain_r, gain_t, *weights)
        back = tp_swap(other)
        pair = (own.astype(jnp.float32) + back.astype(jnp.float32)).astype(jnp.bfloat16)
        kept = pieces(pair[:capacity], cut_back[k])
        for p, piece in enumerate(pieces(pair[capacity:], cut_back[k])):
            cross = member_swap(piece)
            result = (kept[p].astype(jnp.float32) + cross.astype(jnp.float32)).astype(jnp.bfloat16)
            results.append((k * capacity + sum(cut_back[k][:p]), hop(result, k, True)))
    last = experts - 1
    early = [r for r in results if capacity <= r[0] < last * capacity]
    late = [r for r in results if not capacity <= r[0] < last * capacity]
    combined = tail(targets, route_weights, early)
    combined = tail(targets, route_weights, late, combined)
    second_sum = lax.psum(jnp.sum(combined * combined, axis=1), "tp")
    return (combined * lax.rsqrt(second_sum[:, None] / (tp_size * half) + EPS) * out_gain[None, :]).astype(jnp.bfloat16)


def solution(mesh):
    placed = (
        P(("grp", "ep"), "tp"),
        P("tp"),
        P(("grp", "ep"), None),
        P(("grp", "ep"), None),
        P("ep", None, "tp"),
        P("ep", None, "tp"),
        P("ep", "tp", None),
        P("tp"),
    )
    return jax.shard_map(
        per_device, mesh=mesh, in_specs=placed, out_specs=P(("grp", "ep"), "tp"), check_vma=False
    )
```

```python
import functools

import jax
import jax.numpy as jnp
from jax import lax
from jax.experimental import pallas as pl
from jax.experimental.pallas import tpu as pltpu
from jax.sharding import PartitionSpec as P


SPAN_EP = 2
EPS = 1e-06
MIB = 1 << 20


def front_body(home_ref, ids_ref, tok_ref, tgt_ref, *outs, experts, capacity):
    tok_count = tok_ref.shape[0]
    home = home_ref[0]
    ids = ids_ref[...]
    pad = -(-experts // 8) * 8
    expert = lax.broadcasted_iota(jnp.int32, (pad, tok_count), 0)
    hot = [(ids[j : j + 1, :] == expert) for j in range(2)]
    either = (hot[0] | hot[1]).astype(jnp.float32).astype(jnp.bfloat16)
    earlier = (
        lax.broadcasted_iota(jnp.int32, (tok_count, tok_count), 0)
        < lax.broadcasted_iota(jnp.int32, (tok_count, tok_count), 1)
    ).astype(jnp.float32).astype(jnp.bfloat16)
    before = jnp.dot(either, earlier, preferred_element_type=jnp.float32)
    place = []
    for j in range(2):
        slot = jnp.sum(jnp.where(hot[j], before, 0.0), axis=0, keepdims=True).astype(jnp.int32)
        near = nearness(ids[j : j + 1, :], home, experts)
        place.append(near * capacity + slot)
        tgt_ref[j : j + 1, :] = place[j]
    tok = tok_ref[...]
    at = 0
    for out in outs:
        row = lax.broadcasted_iota(jnp.int32, (out.shape[0], tok_count), 0) + at
        at += out.shape[0]
        pick = ((place[0] == row) | (place[1] == row)).astype(jnp.float32).astype(jnp.bfloat16)
        out[...] = jnp.dot(pick, tok, preferred_element_type=jnp.float32).astype(jnp.bfloat16)


def front(home, ids_t, tokens, experts, capacity, sizes):
    tok_count, width = tokens.shape
    vm = pl.BlockSpec(memory_space=pltpu.VMEM)
    return pl.pallas_call(
        functools.partial(front_body, experts=experts, capacity=capacity),
        out_shape=[jax.ShapeDtypeStruct((2, tok_count), jnp.int32)]
        + [jax.ShapeDtypeStruct((size, width), jnp.bfloat16) for size in sizes],
        in_specs=[pl.BlockSpec(memory_space=pltpu.SMEM), vm, vm],
        out_specs=[vm] * (len(sizes) + 1),
        compiler_params=pltpu.CompilerParams(vmem_limit_bytes=12 * MIB),
        name="front",
    )(home, ids_t, tokens)


def nearness(expert, home, experts):
    if experts & (experts - 1) == 0:
        return expert ^ home
    return lax.rem(expert - home + experts, experts)


def sizes_of(capacity, apart):
    first = capacity * 2 // 5 // 16 * 16
    return (first, capacity - first) if apart and first else (capacity,)


def pieces(v, sizes):
    out, at = [], 0
    for size in sizes:
        out.append(v[at : at + size])
        at += size
    return out


def away(home, k, experts):
    if experts & (experts - 1) == 0:
        return home ^ k
    return (home + k) % experts


def cuts_of(units):
    first = -(-units // 256) * 128
    return ((0, first), (first, units - first)) if first < units else ((0, units),)


def normalize(side, rows, gain_m, gain_t, x_v):
    count, at = len(rows) // 2, 0
    for mine_ref, theirs_ref in zip(rows[:count], rows[count:]):
        size, half = mine_ref.shape
        mine = mine_ref[...].astype(jnp.float32)
        theirs = theirs_ref[...].astype(jnp.float32)
        total = jnp.sum(mine * mine, axis=1, keepdims=True) + jnp.sum(theirs * theirs, axis=1, keepdims=True)
        scale = lax.rsqrt(total / (2 * half) + EPS)
        x_v[side, at : at + size] = (mine * scale * gain_m[...]).astype(jnp.bfloat16)
        x_v[1 - side, at : at + size] = (theirs * scale * gain_t[...]).astype(jnp.bfloat16)
        at += size


def ffn_body(side_ref, gain_m, gain_t, wg, wu, wd, *refs):
    rows = refs[:-8]
    own, other, wg_v, wu_v, wd_v, x_v, h_v, sems = refs[-8:]
    half = gain_m.shape[1]
    units = wg_v.shape[1]
    side = side_ref[0]
    cuts = cuts_of(units)
    loads = []
    for at, size in cuts:
        for w, v in ((wg, wg_v), (wu, wu_v)):
            loads.append((w.at[0, :, pl.ds(at, size)], v.at[:, pl.ds(at, size)]))
    for far in (1, 0):
        col = pl.multiple_of((side ^ far) * half, 128)
        loads.append((wd.at[0, :, pl.ds(col, half)], wd_v.at[far]))
    copies = [pltpu.make_async_copy(s, d, sems.at[n]) for n, (s, d) in enumerate(loads)]
    for copy in copies:
        copy.start()
    normalize(side, rows, gain_m, gain_t, x_v)

    def product(w, at, size):
        return jnp.dot(
            x_v[0], w[0:half, at : at + size], preferred_element_type=jnp.float32
        ) + jnp.dot(x_v[1], w[half : 2 * half, at : at + size], preferred_element_type=jnp.float32)

    n = 0
    for at, size in cuts:
        copies[n].wait()
        gate = product(wg_v, at, size)
        copies[n + 1].wait()
        up = product(wu_v, at, size)
        n += 2
        h_v[:, at : at + size] = (gate / (1.0 + jnp.exp(-gate)) * up).astype(jnp.bfloat16)
    hidden = h_v[...]
    for far, out in ((1, other), (0, own)):
        copies[n].wait()
        n += 1
        out[...] = jnp.dot(hidden, wd_v[far], preferred_element_type=jnp.float32).astype(jnp.bfloat16)


def ffn(side, pieces_in, gain_m, gain_t, w_gate, w_up, w_down):
    half = gain_m.shape[1]
    rows = sum(piece.shape[0] for piece in pieces_in) // 2
    units = w_gate.shape[2]
    vm = pl.BlockSpec(memory_space=pltpu.VMEM)
    hbm = pl.BlockSpec(memory_space=pl.ANY)
    out = jax.ShapeDtypeStruct((rows, half), jnp.bfloat16)
    return pl.pallas_call(
        ffn_body,
        out_shape=[out, out],
        in_specs=[pl.BlockSpec(memory_space=pltpu.SMEM), vm, vm, hbm, hbm, hbm] + [vm] * len(pieces_in),
        out_specs=[vm, vm],
        scratch_shapes=[
            pltpu.VMEM((2 * half, units), jnp.bfloat16),
            pltpu.VMEM((2 * half, units), jnp.bfloat16),
            pltpu.VMEM((2, units, half), jnp.bfloat16),
            pltpu.VMEM((2, rows, half), jnp.bfloat16),
            pltpu.VMEM((rows, units), jnp.bfloat16),
            pltpu.SemaphoreType.DMA((2 * len(cuts_of(units)) + 2,)),
        ],
        compiler_params=pltpu.CompilerParams(vmem_limit_bytes=48 * MIB),
        cost_estimate=pl.CostEstimate(
            flops=12 * rows * half * units, transcendentals=rows * units, bytes_accessed=12 * half * units
        ),
        name="ffn",
    )(side, gain_m, gain_t, w_gate, w_up, w_down, *pieces_in)


def resident_body(side_ref, gain_m, gain_t, wg, wu, wd, *refs):
    rows = refs[:-4]
    own, other, x_v, h_v = refs[-4:]
    half = gain_m.shape[1]
    units = wg.shape[2]
    side = side_ref[0]
    normalize(side, rows, gain_m, gain_t, x_v)

    def product(w, at, size):
        return jnp.dot(
            x_v[0], w[0, 0:half, at : at + size], preferred_element_type=jnp.float32
        ) + jnp.dot(x_v[1], w[0, half : 2 * half, at : at + size], preferred_element_type=jnp.float32)

    for at, size in cuts_of(units):
        gate = product(wg, at, size)
        up = product(wu, at, size)
        h_v[:, at : at + size] = (gate / (1.0 + jnp.exp(-gate)) * up).astype(jnp.bfloat16)
    hidden = h_v[...]
    for far, out in ((1, other), (0, own)):
        col = pl.multiple_of((side ^ far) * half, 128)
        out[...] = jnp.dot(
            hidden, wd[0, :, pl.ds(col, half)], preferred_element_type=jnp.float32
        ).astype(jnp.bfloat16)


def resident_ffn(side, pieces_in, gain_m, gain_t, w_gate, w_up, w_down):
    half = gain_m.shape[1]
    rows = sum(piece.shape[0] for piece in pieces_in) // 2
    units = w_gate.shape[2]
    vm = pl.BlockSpec(memory_space=pltpu.VMEM)
    out = jax.ShapeDtypeStruct((rows, half), jnp.bfloat16)
    return pl.pallas_call(
        resident_body,
        out_shape=[out, out],
        in_specs=[pl.BlockSpec(memory_space=pltpu.SMEM)] + [vm] * (5 + len(pieces_in)),
        out_specs=[vm, vm],
        scratch_shapes=[
            pltpu.VMEM((2, rows, half), jnp.bfloat16),
            pltpu.VMEM((rows, units), jnp.bfloat16),
        ],
        compiler_params=pltpu.CompilerParams(vmem_limit_bytes=16 * MIB),
        cost_estimate=pl.CostEstimate(
            flops=12 * rows * half * units, transcendentals=rows * units, bytes_accessed=12 * half * units
        ),
        name="ffn",
    )(side, gain_m, gain_t, w_gate, w_up, w_down, *pieces_in)


def keep_body(wg, wu, wd, *refs):
    refs[-1][...] = refs[0][...]


def keep(value, *weights):
    vm = pl.BlockSpec(memory_space=pltpu.VMEM)
    return pl.pallas_call(
        keep_body,
        out_shape=jax.ShapeDtypeStruct(value.shape, value.dtype),
        in_specs=[vm] * 4,
        out_specs=vm,
        compiler_params=pltpu.CompilerParams(vmem_limit_bytes=16 * MIB),
        name="keep",
    )(*weights, value)


def tail_body(tgt_ref, wts_ref, *refs, places):
    rows, out = refs[: len(places)], refs[-1]
    tok_count = tgt_ref.shape[1]
    total = refs[len(places)][...] if len(refs) > len(places) + 1 else None
    for j in range(2):
        picked = None
        for at, ref in zip(places, rows):
            row = lax.broadcasted_iota(jnp.int32, (ref.shape[0], tok_count), 0) + at
            pick = (tgt_ref[j : j + 1, :] == row).astype(jnp.float32).astype(jnp.bfloat16)
            part = lax.dot_general(
                pick, ref[...], (((0,), (0,)), ((), ())), preferred_element_type=jnp.float32
            )
            picked = part if picked is None else picked + part
        part = picked * wts_ref[:, j : j + 1]
        total = part if total is None else total + part
    out[...] = total


def tail(targets, weights, rows, *total):
    tok_count = targets.shape[1]
    vm = pl.BlockSpec(memory_space=pltpu.VMEM)
    return pl.pallas_call(
        functools.partial(tail_body, places=tuple(at for at, _ in rows)),
        out_shape=jax.ShapeDtypeStruct((tok_count, rows[0][1].shape[1]), jnp.float32),
        in_specs=[vm] * (2 + len(rows) + len(total)),
        out_specs=vm,
        compiler_params=pltpu.CompilerParams(vmem_limit_bytes=12 * MIB),
        name="tail",
    )(targets, weights, *[r for _, r in rows], *total)


def per_device(tokens, in_gain, route_ids, route_weights, w_gate, w_up, w_down, out_gain):
    tok_count, half = tokens.shape
    ep_size = lax.axis_size("ep")
    tp_size = lax.axis_size("tp")
    experts = ep_size // SPAN_EP
    capacity = 2 * (5 * tok_count // (4 * experts))
    home = (lax.axis_index("ep") // SPAN_EP).astype(jnp.int32)
    side = lax.axis_index("tp").astype(jnp.int32).reshape(1)
    swap = [(i, i ^ 1) for i in range(tp_size)]

    def tp_swap(v):
        return lax.ppermute(v, "tp", swap)

    def member_swap(v):
        return lax.ppermute(v, "ep", [(i, i ^ 1) for i in range(ep_size)])

    def hop(v, k, back=False):
        if k == 0:
            return v
        pairs = [
            (e * SPAN_EP + i, away(e, k, experts) * SPAN_EP + i) for e in range(experts) for i in range(SPAN_EP)
        ]
        return lax.ppermute(v, "ep", [(b, a) for a, b in pairs] if back else pairs)

    gain_m = in_gain.reshape(1, half)
    apart = capacity % 32 == 0
    gain_t = tp_swap(gain_m)
    cut_in = [sizes_of(capacity, apart and 2 * k == experts) for k in range(experts)]
    cut_back = [sizes_of(capacity, apart and 2 * k >= experts) for k in range(experts)]
    flat = [size for sizes in cut_in for size in sizes]
    targets, *sent = front(home.reshape(1), route_ids.T, tokens, experts, capacity, flat)
    weights = (w_gate, w_up, w_down)
    gain_m = keep(gain_m, *weights)
    gain_r = keep(gain_m, *weights)
    results = []
    for k in range(experts):
        near = []
        for _ in range(len(cut_in[k])):
            piece = sent.pop(0)
            near.append(hop(piece, k))
        crossed = []
        for piece in near:
            crossed.append(member_swap(piece))
        mine = near + crossed
        theirs = []
        for piece in mine:
            theirs.append(tp_swap(piece))
        if k == 0:
            own, other = ffn(side, mine + theirs, gain_m, gain_t, *weights)
        else:
            own, other = resident_ffn(side, mine + theirs, gain_r, gain_t, *weights)
        back = tp_swap(other)
        pair = (own.astype(jnp.float32) + back.astype(jnp.float32)).astype(jnp.bfloat16)
        kept = pieces(pair[:capacity], cut_back[k])
        for p, piece in enumerate(pieces(pair[capacity:], cut_back[k])):
            cross = member_swap(piece)
            result = (kept[p].astype(jnp.float32) + cross.astype(jnp.float32)).astype(jnp.bfloat16)
            results.append((k * capacity + sum(cut_back[k][:p]), hop(result, k, True)))
    last = experts - 1
    early = [r for r in results if r[0] < last * capacity]
    late = [r for r in results if r[0] >= last * capacity]
    combined = tail(targets, route_weights, early)
    combined = tail(targets, route_weights, late, combined)
    second_sum = lax.psum(jnp.sum(combined * combined, axis=1), "tp")
    return (combined * lax.rsqrt(second_sum[:, None] / (tp_size * half) + EPS) * out_gain[None, :]).astype(jnp.bfloat16)


def solution(mesh):
    placed = (
        P(("grp", "ep"), "tp"),
        P("tp"),
        P(("grp", "ep"), None),
        P(("grp", "ep"), None),
        P("ep", None, "tp"),
        P("ep", None, "tp"),
        P("ep", "tp", None),
        P("tp"),
    )
    return jax.shard_map(
        per_device, mesh=mesh, in_specs=placed, out_specs=P(("grp", "ep"), "tp"), check_vma=False
    )
```

```python
import functools

import jax
import jax.numpy as jnp
from jax import lax
from jax.experimental import pallas as pl
from jax.experimental.pallas import tpu as pltpu
from jax.sharding import PartitionSpec as P


SPAN_EP = 2
EPS = 1e-06
MIB = 1 << 20


def front_body(home_ref, ids_ref, tok_ref, tgt_ref, *outs, experts, capacity):
    tok_count = tok_ref.shape[0]
    home = home_ref[0]
    ids = ids_ref[...]
    pad = -(-experts // 8) * 8
    expert = lax.broadcasted_iota(jnp.int32, (pad, tok_count), 0)
    hot = [(ids[j : j + 1, :] == expert) for j in range(2)]
    either = (hot[0] | hot[1]).astype(jnp.float32).astype(jnp.bfloat16)
    earlier = (
        lax.broadcasted_iota(jnp.int32, (tok_count, tok_count), 0)
        < lax.broadcasted_iota(jnp.int32, (tok_count, tok_count), 1)
    ).astype(jnp.float32).astype(jnp.bfloat16)
    before = jnp.dot(either, earlier, preferred_element_type=jnp.float32)
    place = []
    for j in range(2):
        slot = jnp.sum(jnp.where(hot[j], before, 0.0), axis=0, keepdims=True).astype(jnp.int32)
        near = nearness(ids[j : j + 1, :], home, experts)
        place.append(near * capacity + slot)
        tgt_ref[j : j + 1, :] = place[j]
    tok = tok_ref[...]
    at = 0
    for out in outs:
        row = lax.broadcasted_iota(jnp.int32, (out.shape[0], tok_count), 0) + at
        at += out.shape[0]
        pick = ((place[0] == row) | (place[1] == row)).astype(jnp.float32).astype(jnp.bfloat16)
        out[...] = jnp.dot(pick, tok, preferred_element_type=jnp.float32).astype(jnp.bfloat16)


def front(home, ids_t, tokens, experts, capacity, sizes):
    tok_count, width = tokens.shape
    vm = pl.BlockSpec(memory_space=pltpu.VMEM)
    return pl.pallas_call(
        functools.partial(front_body, experts=experts, capacity=capacity),
        out_shape=[jax.ShapeDtypeStruct((2, tok_count), jnp.int32)]
        + [jax.ShapeDtypeStruct((size, width), jnp.bfloat16) for size in sizes],
        in_specs=[pl.BlockSpec(memory_space=pltpu.SMEM), vm, vm],
        out_specs=[vm] * (len(sizes) + 1),
        compiler_params=pltpu.CompilerParams(vmem_limit_bytes=12 * MIB),
        name="front",
    )(home, ids_t, tokens)


def nearness(expert, home, experts):
    if experts & (experts - 1) == 0:
        return expert ^ home
    return lax.rem(expert - home + experts, experts)


def sizes_of(capacity, apart):
    first = capacity * 2 // 5 // 16 * 16
    return (first, capacity - first) if apart and first else (capacity,)


def pieces(v, sizes):
    out, at = [], 0
    for size in sizes:
        out.append(v[at : at + size])
        at += size
    return out


def away(home, k, experts):
    if experts & (experts - 1) == 0:
        return home ^ k
    return (home + k) % experts


def cuts_of(units):
    first = -(-units // 256) * 128
    return ((0, first), (first, units - first)) if first < units else ((0, units),)


def normalize(side, rows, gain_m, gain_t, x_v):
    count, at = len(rows) // 2, 0
    for mine_ref, theirs_ref in zip(rows[:count], rows[count:]):
        size, half = mine_ref.shape
        mine = mine_ref[...].astype(jnp.float32)
        theirs = theirs_ref[...].astype(jnp.float32)
        total = jnp.sum(mine * mine, axis=1, keepdims=True) + jnp.sum(theirs * theirs, axis=1, keepdims=True)
        scale = lax.rsqrt(total / (2 * half) + EPS)
        x_v[side, at : at + size] = (mine * scale * gain_m[...]).astype(jnp.bfloat16)
        x_v[1 - side, at : at + size] = (theirs * scale * gain_t[...]).astype(jnp.bfloat16)
        at += size


def ffn_body(side_ref, gain_m, gain_t, wg, wu, wd, *refs):
    rows = refs[:-8]
    own, other, wg_v, wu_v, wd_v, x_v, h_v, sems = refs[-8:]
    half = gain_m.shape[1]
    units = wg_v.shape[1]
    side = side_ref[0]
    cuts = cuts_of(units)
    loads = []
    for at, size in cuts:
        for w, v in ((wg, wg_v), (wu, wu_v)):
            loads.append((w.at[0, :, pl.ds(at, size)], v.at[:, pl.ds(at, size)]))
    for far in (1, 0):
        col = pl.multiple_of((side ^ far) * half, 128)
        loads.append((wd.at[0, :, pl.ds(col, half)], wd_v.at[far]))
    copies = [pltpu.make_async_copy(s, d, sems.at[n]) for n, (s, d) in enumerate(loads)]
    for copy in copies:
        copy.start()
    normalize(side, rows, gain_m, gain_t, x_v)

    def product(w, at, size):
        return jnp.dot(
            x_v[0], w[0:half, at : at + size], preferred_element_type=jnp.float32
        ) + jnp.dot(x_v[1], w[half : 2 * half, at : at + size], preferred_element_type=jnp.float32)

    n = 0
    for at, size in cuts:
        copies[n].wait()
        gate = product(wg_v, at, size)
        copies[n + 1].wait()
        up = product(wu_v, at, size)
        n += 2
        h_v[:, at : at + size] = (gate / (1.0 + jnp.exp(-gate)) * up).astype(jnp.bfloat16)
    hidden = h_v[...]
    for far, out in ((1, other), (0, own)):
        copies[n].wait()
        n += 1
        out[...] = jnp.dot(hidden, wd_v[far], preferred_element_type=jnp.float32).astype(jnp.bfloat16)


def ffn(side, pieces_in, gain_m, gain_t, w_gate, w_up, w_down):
    half = gain_m.shape[1]
    rows = sum(piece.shape[0] for piece in pieces_in) // 2
    units = w_gate.shape[2]
    vm = pl.BlockSpec(memory_space=pltpu.VMEM)
    hbm = pl.BlockSpec(memory_space=pl.ANY)
    out = jax.ShapeDtypeStruct((rows, half), jnp.bfloat16)
    return pl.pallas_call(
        ffn_body,
        out_shape=[out, out],
        in_specs=[pl.BlockSpec(memory_space=pltpu.SMEM), vm, vm, hbm, hbm, hbm] + [vm] * len(pieces_in),
        out_specs=[vm, vm],
        scratch_shapes=[
            pltpu.VMEM((2 * half, units), jnp.bfloat16),
            pltpu.VMEM((2 * half, units), jnp.bfloat16),
            pltpu.VMEM((2, units, half), jnp.bfloat16),
            pltpu.VMEM((2, rows, half), jnp.bfloat16),
            pltpu.VMEM((rows, units), jnp.bfloat16),
            pltpu.SemaphoreType.DMA((2 * len(cuts_of(units)) + 2,)),
        ],
        compiler_params=pltpu.CompilerParams(vmem_limit_bytes=48 * MIB),
        cost_estimate=pl.CostEstimate(
            flops=12 * rows * half * units, transcendentals=rows * units, bytes_accessed=12 * half * units
        ),
        name="ffn",
    )(side, gain_m, gain_t, w_gate, w_up, w_down, *pieces_in)


def resident_body(side_ref, gain_m, gain_t, wg, wu, wd, *refs):
    rows = refs[:-4]
    own, other, x_v, h_v = refs[-4:]
    half = gain_m.shape[1]
    units = wg.shape[2]
    side = side_ref[0]
    normalize(side, rows, gain_m, gain_t, x_v)

    def product(w, at, size):
        return jnp.dot(
            x_v[0], w[0, 0:half, at : at + size], preferred_element_type=jnp.float32
        ) + jnp.dot(x_v[1], w[0, half : 2 * half, at : at + size], preferred_element_type=jnp.float32)

    for at, size in cuts_of(units):
        gate = product(wg, at, size)
        up = product(wu, at, size)
        h_v[:, at : at + size] = (gate / (1.0 + jnp.exp(-gate)) * up).astype(jnp.bfloat16)
    hidden = h_v[...]
    for far, out in ((1, other), (0, own)):
        col = pl.multiple_of((side ^ far) * half, 128)
        out[...] = jnp.dot(
            hidden, wd[0, :, pl.ds(col, half)], preferred_element_type=jnp.float32
        ).astype(jnp.bfloat16)


def resident_ffn(side, pieces_in, gain_m, gain_t, w_gate, w_up, w_down):
    half = gain_m.shape[1]
    rows = sum(piece.shape[0] for piece in pieces_in) // 2
    units = w_gate.shape[2]
    vm = pl.BlockSpec(memory_space=pltpu.VMEM)
    out = jax.ShapeDtypeStruct((rows, half), jnp.bfloat16)
    return pl.pallas_call(
        resident_body,
        out_shape=[out, out],
        in_specs=[pl.BlockSpec(memory_space=pltpu.SMEM)] + [vm] * (5 + len(pieces_in)),
        out_specs=[vm, vm],
        scratch_shapes=[
            pltpu.VMEM((2, rows, half), jnp.bfloat16),
            pltpu.VMEM((rows, units), jnp.bfloat16),
        ],
        compiler_params=pltpu.CompilerParams(vmem_limit_bytes=16 * MIB),
        cost_estimate=pl.CostEstimate(
            flops=12 * rows * half * units, transcendentals=rows * units, bytes_accessed=12 * half * units
        ),
        name="ffn",
    )(side, gain_m, gain_t, w_gate, w_up, w_down, *pieces_in)


def keep_body(wg, wu, wd, *refs):
    refs[-1][...] = refs[0][...]


def keep(value, *weights):
    vm = pl.BlockSpec(memory_space=pltpu.VMEM)
    return pl.pallas_call(
        keep_body,
        out_shape=jax.ShapeDtypeStruct(value.shape, value.dtype),
        in_specs=[vm] * 4,
        out_specs=vm,
        compiler_params=pltpu.CompilerParams(vmem_limit_bytes=16 * MIB),
        name="keep",
    )(*weights, value)


def tail_body(tgt_ref, wts_ref, *refs, places):
    rows, out = refs[: len(places)], refs[-1]
    tok_count = tgt_ref.shape[1]
    total = refs[len(places)][...] if len(refs) > len(places) + 1 else None
    for j in range(2):
        picked = None
        for at, ref in zip(places, rows):
            row = lax.broadcasted_iota(jnp.int32, (ref.shape[0], tok_count), 0) + at
            pick = (tgt_ref[j : j + 1, :] == row).astype(jnp.float32).astype(jnp.bfloat16)
            part = lax.dot_general(
                pick, ref[...], (((0,), (0,)), ((), ())), preferred_element_type=jnp.float32
            )
            picked = part if picked is None else picked + part
        part = picked * wts_ref[:, j : j + 1]
        total = part if total is None else total + part
    out[...] = total


def tail(targets, weights, rows, *total):
    tok_count = targets.shape[1]
    vm = pl.BlockSpec(memory_space=pltpu.VMEM)
    return pl.pallas_call(
        functools.partial(tail_body, places=tuple(at for at, _ in rows)),
        out_shape=jax.ShapeDtypeStruct((tok_count, rows[0][1].shape[1]), jnp.float32),
        in_specs=[vm] * (2 + len(rows) + len(total)),
        out_specs=vm,
        compiler_params=pltpu.CompilerParams(vmem_limit_bytes=12 * MIB),
        name="tail",
    )(targets, weights, *[r for _, r in rows], *total)


def per_device(tokens, in_gain, route_ids, route_weights, w_gate, w_up, w_down, out_gain):
    tok_count, half = tokens.shape
    ep_size = lax.axis_size("ep")
    tp_size = lax.axis_size("tp")
    experts = ep_size // SPAN_EP
    capacity = 2 * (5 * tok_count // (4 * experts))
    home = (lax.axis_index("ep") // SPAN_EP).astype(jnp.int32)
    side = lax.axis_index("tp").astype(jnp.int32).reshape(1)
    swap = [(i, i ^ 1) for i in range(tp_size)]

    def tp_swap(v):
        return lax.ppermute(v, "tp", swap)

    def member_swap(v):
        return lax.ppermute(v, "ep", [(i, i ^ 1) for i in range(ep_size)])

    def hop(v, k, back=False):
        if k == 0:
            return v
        pairs = [
            (e * SPAN_EP + i, away(e, k, experts) * SPAN_EP + i) for e in range(experts) for i in range(SPAN_EP)
        ]
        return lax.ppermute(v, "ep", [(b, a) for a, b in pairs] if back else pairs)

    gain_m = in_gain.reshape(1, half)
    apart = capacity % 32 == 0
    gain_t = tp_swap(gain_m)
    cut_in = [sizes_of(capacity, apart and 2 * k == experts) for k in range(experts)]
    cut_back = [sizes_of(capacity, apart and k > 0) for k in range(experts)]
    flat = [size for sizes in cut_in for size in sizes]
    targets, *sent = front(home.reshape(1), route_ids.T, tokens, experts, capacity, flat)
    weights = (w_gate, w_up, w_down)
    gain_m = keep(gain_m, *weights)
    gain_r = keep(gain_m, *weights)
    results = []
    for k in range(experts):
        near = []
        for _ in range(len(cut_in[k])):
            piece = sent.pop(0)
            near.append(hop(piece, k))
        crossed = []
        for piece in near:
            crossed.append(member_swap(piece))
        mine = near + crossed
        theirs = []
        for piece in mine:
            theirs.append(tp_swap(piece))
        if k == 0:
            own, other = ffn(side, mine + theirs, gain_m, gain_t, *weights)
        else:
            own, other = resident_ffn(side, mine + theirs, gain_r, gain_t, *weights)
        back = tp_swap(other)
        pair = (own.astype(jnp.float32) + back.astype(jnp.float32)).astype(jnp.bfloat16)
        kept = pieces(pair[:capacity], cut_back[k])
        for p, piece in enumerate(pieces(pair[capacity:], cut_back[k])):
            cross = member_swap(piece)
            result = (kept[p].astype(jnp.float32) + cross.astype(jnp.float32)).astype(jnp.bfloat16)
            results.append((k * capacity + sum(cut_back[k][:p]), hop(result, k, True)))
    near = [capacity <= at < 2 * capacity for at, _ in results]
    early = [r for r, n in zip(results, near) if not n]
    late = [r for r, n in zip(results, near) if n]
    combined = tail(targets, route_weights, early)
    combined = tail(targets, route_weights, late, combined)
    second_sum = lax.psum(jnp.sum(combined * combined, axis=1), "tp")
    return (combined * lax.rsqrt(second_sum[:, None] / (tp_size * half) + EPS) * out_gain[None, :]).astype(jnp.bfloat16)


def solution(mesh):
    placed = (
        P(("grp", "ep"), "tp"),
        P("tp"),
        P(("grp", "ep"), None),
        P(("grp", "ep"), None),
        P("ep", None, "tp"),
        P("ep", None, "tp"),
        P("ep", "tp", None),
        P("tp"),
    )
    return jax.shard_map(
        per_device, mesh=mesh, in_specs=placed, out_specs=P(("grp", "ep"), "tp"), check_vma=False
    )
```

```python
import functools

import jax
import jax.numpy as jnp
from jax import lax
from jax.experimental import pallas as pl
from jax.experimental.pallas import tpu as pltpu
from jax.sharding import PartitionSpec as P


SPAN_EP = 2
EPS = 1e-06
MIB = 1 << 20


def front_body(home_ref, ids_ref, tok_ref, tgt_ref, *outs, experts, capacity):
    tok_count = tok_ref.shape[0]
    home = home_ref[0]
    ids = ids_ref[...]
    pad = -(-experts // 8) * 8
    expert = lax.broadcasted_iota(jnp.int32, (pad, tok_count), 0)
    hot = [(ids[j : j + 1, :] == expert) for j in range(2)]
    either = (hot[0] | hot[1]).astype(jnp.float32).astype(jnp.bfloat16)
    earlier = (
        lax.broadcasted_iota(jnp.int32, (tok_count, tok_count), 0)
        < lax.broadcasted_iota(jnp.int32, (tok_count, tok_count), 1)
    ).astype(jnp.float32).astype(jnp.bfloat16)
    before = jnp.dot(either, earlier, preferred_element_type=jnp.float32)
    place = []
    for j in range(2):
        slot = jnp.sum(jnp.where(hot[j], before, 0.0), axis=0, keepdims=True).astype(jnp.int32)
        near = nearness(ids[j : j + 1, :], home, experts)
        place.append(near * capacity + slot)
        tgt_ref[j : j + 1, :] = place[j]
    tok = tok_ref[...]
    at = 0
    for out in outs:
        row = lax.broadcasted_iota(jnp.int32, (out.shape[0], tok_count), 0) + at
        at += out.shape[0]
        pick = ((place[0] == row) | (place[1] == row)).astype(jnp.float32).astype(jnp.bfloat16)
        out[...] = jnp.dot(pick, tok, preferred_element_type=jnp.float32).astype(jnp.bfloat16)


def front(home, ids_t, tokens, experts, capacity, sizes):
    tok_count, width = tokens.shape
    vm = pl.BlockSpec(memory_space=pltpu.VMEM)
    return pl.pallas_call(
        functools.partial(front_body, experts=experts, capacity=capacity),
        out_shape=[jax.ShapeDtypeStruct((2, tok_count), jnp.int32)]
        + [jax.ShapeDtypeStruct((size, width), jnp.bfloat16) for size in sizes],
        in_specs=[pl.BlockSpec(memory_space=pltpu.SMEM), vm, vm],
        out_specs=[vm] * (len(sizes) + 1),
        compiler_params=pltpu.CompilerParams(vmem_limit_bytes=12 * MIB),
        name="front",
    )(home, ids_t, tokens)


def nearness(expert, home, experts):
    if experts & (experts - 1) == 0:
        return expert ^ home
    return lax.rem(expert - home + experts, experts)


def away(home, k, experts):
    if experts & (experts - 1) == 0:
        return home ^ k
    return (home + k) % experts


def cuts_of(units):
    first = -(-units // 256) * 128
    return ((0, first), (first, units - first)) if first < units else ((0, units),)


def normalize(side, rows, gain_m, gain_t, x_v):
    count, at = len(rows) // 2, 0
    for mine_ref, theirs_ref in zip(rows[:count], rows[count:]):
        size, half = mine_ref.shape
        mine = mine_ref[...].astype(jnp.float32)
        theirs = theirs_ref[...].astype(jnp.float32)
        total = jnp.sum(mine * mine, axis=1, keepdims=True) + jnp.sum(theirs * theirs, axis=1, keepdims=True)
        scale = lax.rsqrt(total / (2 * half) + EPS)
        x_v[side, at : at + size] = (mine * scale * gain_m[...]).astype(jnp.bfloat16)
        x_v[1 - side, at : at + size] = (theirs * scale * gain_t[...]).astype(jnp.bfloat16)
        at += size


def ffn_body(side_ref, gain_m, gain_t, wg, wu, wd, *refs):
    rows = refs[:-8]
    own, other, wg_v, wu_v, wd_v, x_v, h_v, sems = refs[-8:]
    half = gain_m.shape[1]
    units = wg_v.shape[1]
    side = side_ref[0]
    cuts = cuts_of(units)
    loads = []
    for at, size in cuts:
        for w, v in ((wg, wg_v), (wu, wu_v)):
            loads.append((w.at[0, :, pl.ds(at, size)], v.at[:, pl.ds(at, size)]))
    for far in (1, 0):
        col = pl.multiple_of((side ^ far) * half, 128)
        loads.append((wd.at[0, :, pl.ds(col, half)], wd_v.at[far]))
    copies = [pltpu.make_async_copy(s, d, sems.at[n]) for n, (s, d) in enumerate(loads)]
    for copy in copies:
        copy.start()
    normalize(side, rows, gain_m, gain_t, x_v)

    def product(w, at, size):
        return jnp.dot(
            x_v[0], w[0:half, at : at + size], preferred_element_type=jnp.float32
        ) + jnp.dot(x_v[1], w[half : 2 * half, at : at + size], preferred_element_type=jnp.float32)

    n = 0
    for at, size in cuts:
        copies[n].wait()
        gate = product(wg_v, at, size)
        copies[n + 1].wait()
        up = product(wu_v, at, size)
        n += 2
        h_v[:, at : at + size] = (gate / (1.0 + jnp.exp(-gate)) * up).astype(jnp.bfloat16)
    hidden = h_v[...]
    for far, out in ((1, other), (0, own)):
        copies[n].wait()
        n += 1
        out[...] = jnp.dot(hidden, wd_v[far], preferred_element_type=jnp.float32).astype(jnp.bfloat16)


def ffn(side, pieces_in, gain_m, gain_t, w_gate, w_up, w_down):
    half = gain_m.shape[1]
    rows = sum(piece.shape[0] for piece in pieces_in) // 2
    units = w_gate.shape[2]
    vm = pl.BlockSpec(memory_space=pltpu.VMEM)
    hbm = pl.BlockSpec(memory_space=pl.ANY)
    out = jax.ShapeDtypeStruct((rows, half), jnp.bfloat16)
    return pl.pallas_call(
        ffn_body,
        out_shape=[out, out],
        in_specs=[pl.BlockSpec(memory_space=pltpu.SMEM), vm, vm, hbm, hbm, hbm] + [vm] * len(pieces_in),
        out_specs=[vm, vm],
        scratch_shapes=[
            pltpu.VMEM((2 * half, units), jnp.bfloat16),
            pltpu.VMEM((2 * half, units), jnp.bfloat16),
            pltpu.VMEM((2, units, half), jnp.bfloat16),
            pltpu.VMEM((2, rows, half), jnp.bfloat16),
            pltpu.VMEM((rows, units), jnp.bfloat16),
            pltpu.SemaphoreType.DMA((2 * len(cuts_of(units)) + 2,)),
        ],
        compiler_params=pltpu.CompilerParams(vmem_limit_bytes=51 * MIB),
        cost_estimate=pl.CostEstimate(
            flops=12 * rows * half * units, transcendentals=rows * units, bytes_accessed=12 * half * units
        ),
        name="ffn",
    )(side, gain_m, gain_t, w_gate, w_up, w_down, *pieces_in)


def resident_body(side_ref, gain_m, gain_t, wg, wu, wd, *refs):
    rows = refs[:-4]
    own, other, x_v, h_v = refs[-4:]
    half = gain_m.shape[1]
    units = wg.shape[2]
    side = side_ref[0]
    normalize(side, rows, gain_m, gain_t, x_v)

    def product(w, at, size):
        return jnp.dot(
            x_v[0], w[0, 0:half, at : at + size], preferred_element_type=jnp.float32
        ) + jnp.dot(x_v[1], w[0, half : 2 * half, at : at + size], preferred_element_type=jnp.float32)

    for at, size in cuts_of(units):
        gate = product(wg, at, size)
        up = product(wu, at, size)
        h_v[:, at : at + size] = (gate / (1.0 + jnp.exp(-gate)) * up).astype(jnp.bfloat16)
    hidden = h_v[...]
    for far, out in ((1, other), (0, own)):
        col = pl.multiple_of((side ^ far) * half, 128)
        out[...] = jnp.dot(
            hidden, wd[0, :, pl.ds(col, half)], preferred_element_type=jnp.float32
        ).astype(jnp.bfloat16)


def resident_ffn(side, pieces_in, gain_m, gain_t, w_gate, w_up, w_down):
    half = gain_m.shape[1]
    rows = sum(piece.shape[0] for piece in pieces_in) // 2
    units = w_gate.shape[2]
    vm = pl.BlockSpec(memory_space=pltpu.VMEM)
    out = jax.ShapeDtypeStruct((rows, half), jnp.bfloat16)
    return pl.pallas_call(
        resident_body,
        out_shape=[out, out],
        in_specs=[pl.BlockSpec(memory_space=pltpu.SMEM)] + [vm] * (5 + len(pieces_in)),
        out_specs=[vm, vm],
        scratch_shapes=[
            pltpu.VMEM((2, rows, half), jnp.bfloat16),
            pltpu.VMEM((rows, units), jnp.bfloat16),
        ],
        compiler_params=pltpu.CompilerParams(vmem_limit_bytes=16 * MIB),
        cost_estimate=pl.CostEstimate(
            flops=12 * rows * half * units, transcendentals=rows * units, bytes_accessed=12 * half * units
        ),
        name="ffn",
    )(side, gain_m, gain_t, w_gate, w_up, w_down, *pieces_in)


def keep_body(wg, wu, wd, *refs):
    refs[-1][...] = refs[0][...]


def keep(value, *weights):
    vm = pl.BlockSpec(memory_space=pltpu.VMEM)
    return pl.pallas_call(
        keep_body,
        out_shape=jax.ShapeDtypeStruct(value.shape, value.dtype),
        in_specs=[vm] * 4,
        out_specs=vm,
        compiler_params=pltpu.CompilerParams(vmem_limit_bytes=16 * MIB),
        name="keep",
    )(*weights, value)


def tail_body(tgt_ref, wts_ref, *refs, places):
    rows, out = refs[: len(places)], refs[-1]
    tok_count = tgt_ref.shape[1]
    total = refs[len(places)][...] if len(refs) > len(places) + 1 else None
    for j in range(2):
        picked = None
        for at, ref in zip(places, rows):
            row = lax.broadcasted_iota(jnp.int32, (ref.shape[0], tok_count), 0) + at
            pick = (tgt_ref[j : j + 1, :] == row).astype(jnp.float32).astype(jnp.bfloat16)
            part = lax.dot_general(
                pick, ref[...], (((0,), (0,)), ((), ())), preferred_element_type=jnp.float32
            )
            picked = part if picked is None else picked + part
        part = picked * wts_ref[:, j : j + 1]
        total = part if total is None else total + part
    out[...] = total


def tail(targets, weights, rows, *total):
    tok_count = targets.shape[1]
    vm = pl.BlockSpec(memory_space=pltpu.VMEM)
    return pl.pallas_call(
        functools.partial(tail_body, places=tuple(at for at, _ in rows)),
        out_shape=jax.ShapeDtypeStruct((tok_count, rows[0][1].shape[1]), jnp.float32),
        in_specs=[vm] * (2 + len(rows) + len(total)),
        out_specs=vm,
        compiler_params=pltpu.CompilerParams(vmem_limit_bytes=12 * MIB),
        name="tail",
    )(targets, weights, *[r for _, r in rows], *total)


def per_device(tokens, in_gain, route_ids, route_weights, w_gate, w_up, w_down, out_gain):
    tok_count, half = tokens.shape
    ep_size = lax.axis_size("ep")
    tp_size = lax.axis_size("tp")
    experts = ep_size // SPAN_EP
    capacity = 2 * (5 * tok_count // (4 * experts))
    home = (lax.axis_index("ep") // SPAN_EP).astype(jnp.int32)
    side = lax.axis_index("tp").astype(jnp.int32).reshape(1)
    swap = [(i, i ^ 1) for i in range(tp_size)]

    def tp_swap(v):
        return lax.ppermute(v, "tp", swap)

    def member_swap(v):
        return lax.ppermute(v, "ep", [(i, i ^ 1) for i in range(ep_size)])

    def hop(v, k, back=False):
        if k == 0:
            return v
        pairs = [
            (e * SPAN_EP + i, away(e, k, experts) * SPAN_EP + i) for e in range(experts) for i in range(SPAN_EP)
        ]
        return lax.ppermute(v, "ep", [(b, a) for a, b in pairs] if back else pairs)

    gain_m = in_gain.reshape(1, half)
    gain_t = tp_swap(gain_m)
    targets, *sent = front(home.reshape(1), route_ids.T, tokens, experts, capacity, [capacity] * experts)
    weights = (w_gate, w_up, w_down)
    gain_m = keep(gain_m, *weights)
    gain_r = keep(gain_m, *weights)
    results = []
    for k in range(experts):
        near = hop(sent[k], k)
        crossed = member_swap(near)
        mine = [near, crossed]
        theirs = []
        for piece in mine:
            theirs.append(tp_swap(piece))
        if k == 0:
            own, other = ffn(side, mine + theirs, gain_m, gain_t, *weights)
        else:
            own, other = resident_ffn(side, mine + theirs, gain_r, gain_t, *weights)
        back = tp_swap(other)
        pair = (own.astype(jnp.float32) + back.astype(jnp.float32)).astype(jnp.bfloat16)
        cross = member_swap(pair[capacity:])
        result = (pair[:capacity].astype(jnp.float32) + cross.astype(jnp.float32)).astype(jnp.bfloat16)
        results.append((k * capacity, hop(result, k, True)))
    middle = experts // 2 * capacity
    early = [r for r in results if r[0] >= middle]
    late = [r for r in results if r[0] < middle]
    combined = tail(targets, route_weights, early)
    combined = tail(targets, route_weights, late, combined)
    second_sum = lax.psum(jnp.sum(combined * combined, axis=1), "tp")
    return (combined * lax.rsqrt(second_sum[:, None] / (tp_size * half) + EPS) * out_gain[None, :]).astype(jnp.bfloat16)


def solution(mesh):
    placed = (
        P(("grp", "ep"), "tp"),
        P("tp"),
        P(("grp", "ep"), None),
        P(("grp", "ep"), None),
        P("ep", None, "tp"),
        P("ep", None, "tp"),
        P("ep", "tp", None),
        P("tp"),
    )
    return jax.shard_map(
        per_device, mesh=mesh, in_specs=placed, out_specs=P(("grp", "ep"), "tp"), check_vma=False
    )
```

```python
import functools

import jax
import jax.numpy as jnp
from jax import lax
from jax.experimental import pallas as pl
from jax.experimental.pallas import tpu as pltpu
from jax.sharding import PartitionSpec as P


SPAN_EP = 2
EPS = 1e-06
MIB = 1 << 20


def front_body(home_ref, ids_ref, tok_ref, tgt_ref, *outs, experts, capacity):
    tok_count = tok_ref.shape[0]
    home = home_ref[0]
    ids = ids_ref[...]
    pad = -(-experts // 8) * 8
    expert = lax.broadcasted_iota(jnp.int32, (pad, tok_count), 0)
    hot = [(ids[j : j + 1, :] == expert) for j in range(2)]
    either = (hot[0] | hot[1]).astype(jnp.float32).astype(jnp.bfloat16)
    earlier = (
        lax.broadcasted_iota(jnp.int32, (tok_count, tok_count), 0)
        < lax.broadcasted_iota(jnp.int32, (tok_count, tok_count), 1)
    ).astype(jnp.float32).astype(jnp.bfloat16)
    before = jnp.dot(either, earlier, preferred_element_type=jnp.float32)
    place = []
    for j in range(2):
        slot = jnp.sum(jnp.where(hot[j], before, 0.0), axis=0, keepdims=True).astype(jnp.int32)
        near = nearness(ids[j : j + 1, :], home, experts)
        place.append(near * capacity + slot)
        tgt_ref[j : j + 1, :] = place[j]
    tok = tok_ref[...]
    at = 0
    for out in outs:
        row = lax.broadcasted_iota(jnp.int32, (out.shape[0], tok_count), 0) + at
        at += out.shape[0]
        pick = ((place[0] == row) | (place[1] == row)).astype(jnp.float32).astype(jnp.bfloat16)
        out[...] = jnp.dot(pick, tok, preferred_element_type=jnp.float32).astype(jnp.bfloat16)


def front(home, ids_t, tokens, experts, capacity, sizes):
    tok_count, width = tokens.shape
    vm = pl.BlockSpec(memory_space=pltpu.VMEM)
    return pl.pallas_call(
        functools.partial(front_body, experts=experts, capacity=capacity),
        out_shape=[jax.ShapeDtypeStruct((2, tok_count), jnp.int32)]
        + [jax.ShapeDtypeStruct((size, width), jnp.bfloat16) for size in sizes],
        in_specs=[pl.BlockSpec(memory_space=pltpu.SMEM), vm, vm],
        out_specs=[vm] * (len(sizes) + 1),
        compiler_params=pltpu.CompilerParams(vmem_limit_bytes=12 * MIB),
        name="front",
    )(home, ids_t, tokens)


def nearness(expert, home, experts):
    if experts & (experts - 1) == 0:
        return expert ^ home
    return lax.rem(expert - home + experts, experts)


def sizes_of(capacity, apart):
    first = capacity * 2 // 5 // 16 * 16
    return (first, capacity - first) if apart and first else (capacity,)


def pieces(v, sizes):
    out, at = [], 0
    for size in sizes:
        out.append(v[at : at + size])
        at += size
    return out


def away(home, k, experts):
    if experts & (experts - 1) == 0:
        return home ^ k
    return (home + k) % experts


def cuts_of(units):
    first = -(-units // 256) * 128
    return ((0, first), (first, units - first)) if first < units else ((0, units),)


def normalize(side, rows, gain_m, gain_t, x_v):
    count, at = len(rows) // 2, 0
    for mine_ref, theirs_ref in zip(rows[:count], rows[count:]):
        size, half = mine_ref.shape
        mine = mine_ref[...].astype(jnp.float32)
        theirs = theirs_ref[...].astype(jnp.float32)
        total = jnp.sum(mine * mine, axis=1, keepdims=True) + jnp.sum(theirs * theirs, axis=1, keepdims=True)
        scale = lax.rsqrt(total / (2 * half) + EPS)
        x_v[side, at : at + size] = (mine * scale * gain_m[...]).astype(jnp.bfloat16)
        x_v[1 - side, at : at + size] = (theirs * scale * gain_t[...]).astype(jnp.bfloat16)
        at += size


def ffn_body(side_ref, gain_m, gain_t, wg, wu, wd, *refs):
    rows = refs[:-8]
    own, other, wg_v, wu_v, wd_v, x_v, h_v, sems = refs[-8:]
    half = gain_m.shape[1]
    units = wg_v.shape[1]
    side = side_ref[0]
    cuts = cuts_of(units)
    loads = []
    for at, size in cuts:
        for w, v in ((wg, wg_v), (wu, wu_v)):
            loads.append((w.at[0, :, pl.ds(at, size)], v.at[:, pl.ds(at, size)]))
    for far in (1, 0):
        col = pl.multiple_of((side ^ far) * half, 128)
        loads.append((wd.at[0, :, pl.ds(col, half)], wd_v.at[far]))
    copies = [pltpu.make_async_copy(s, d, sems.at[n]) for n, (s, d) in enumerate(loads)]
    for copy in copies:
        copy.start()
    normalize(side, rows, gain_m, gain_t, x_v)

    def product(w, at, size):
        return jnp.dot(
            x_v[0], w[0:half, at : at + size], preferred_element_type=jnp.float32
        ) + jnp.dot(x_v[1], w[half : 2 * half, at : at + size], preferred_element_type=jnp.float32)

    n = 0
    for at, size in cuts:
        copies[n].wait()
        gate = product(wg_v, at, size)
        copies[n + 1].wait()
        up = product(wu_v, at, size)
        n += 2
        h_v[:, at : at + size] = (gate / (1.0 + jnp.exp(-gate)) * up).astype(jnp.bfloat16)
    hidden = h_v[...]
    for far, out in ((1, other), (0, own)):
        copies[n].wait()
        n += 1
        out[...] = jnp.dot(hidden, wd_v[far], preferred_element_type=jnp.float32).astype(jnp.bfloat16)


def ffn(side, pieces_in, gain_m, gain_t, w_gate, w_up, w_down):
    half = gain_m.shape[1]
    rows = sum(piece.shape[0] for piece in pieces_in) // 2
    units = w_gate.shape[2]
    vm = pl.BlockSpec(memory_space=pltpu.VMEM)
    hbm = pl.BlockSpec(memory_space=pl.ANY)
    out = jax.ShapeDtypeStruct((rows, half), jnp.bfloat16)
    return pl.pallas_call(
        ffn_body,
        out_shape=[out, out],
        in_specs=[pl.BlockSpec(memory_space=pltpu.SMEM), vm, vm, hbm, hbm, hbm] + [vm] * len(pieces_in),
        out_specs=[vm, vm],
        scratch_shapes=[
            pltpu.VMEM((2 * half, units), jnp.bfloat16),
            pltpu.VMEM((2 * half, units), jnp.bfloat16),
            pltpu.VMEM((2, units, half), jnp.bfloat16),
            pltpu.VMEM((2, rows, half), jnp.bfloat16),
            pltpu.VMEM((rows, units), jnp.bfloat16),
            pltpu.SemaphoreType.DMA((2 * len(cuts_of(units)) + 2,)),
        ],
        compiler_params=pltpu.CompilerParams(vmem_limit_bytes=48 * MIB),
        cost_estimate=pl.CostEstimate(
            flops=12 * rows * half * units, transcendentals=rows * units, bytes_accessed=12 * half * units
        ),
        name="ffn",
    )(side, gain_m, gain_t, w_gate, w_up, w_down, *pieces_in)


def resident_body(side_ref, gain_m, gain_t, wg, wu, wd, *refs):
    rows = refs[:-4]
    own, other, x_v, h_v = refs[-4:]
    half = gain_m.shape[1]
    units = wg.shape[2]
    side = side_ref[0]
    normalize(side, rows, gain_m, gain_t, x_v)

    def product(w, at, size):
        return jnp.dot(
            x_v[0], w[0, 0:half, at : at + size], preferred_element_type=jnp.float32
        ) + jnp.dot(x_v[1], w[0, half : 2 * half, at : at + size], preferred_element_type=jnp.float32)

    for at, size in cuts_of(units):
        gate = product(wg, at, size)
        up = product(wu, at, size)
        h_v[:, at : at + size] = (gate / (1.0 + jnp.exp(-gate)) * up).astype(jnp.bfloat16)
    hidden = h_v[...]
    for far, out in ((1, other), (0, own)):
        col = pl.multiple_of((side ^ far) * half, 128)
        out[...] = jnp.dot(
            hidden, wd[0, :, pl.ds(col, half)], preferred_element_type=jnp.float32
        ).astype(jnp.bfloat16)


def resident_ffn(side, pieces_in, gain_m, gain_t, w_gate, w_up, w_down):
    half = gain_m.shape[1]
    rows = sum(piece.shape[0] for piece in pieces_in) // 2
    units = w_gate.shape[2]
    vm = pl.BlockSpec(memory_space=pltpu.VMEM)
    out = jax.ShapeDtypeStruct((rows, half), jnp.bfloat16)
    return pl.pallas_call(
        resident_body,
        out_shape=[out, out],
        in_specs=[pl.BlockSpec(memory_space=pltpu.SMEM)] + [vm] * (5 + len(pieces_in)),
        out_specs=[vm, vm],
        scratch_shapes=[
            pltpu.VMEM((2, rows, half), jnp.bfloat16),
            pltpu.VMEM((rows, units), jnp.bfloat16),
        ],
        compiler_params=pltpu.CompilerParams(vmem_limit_bytes=16 * MIB),
        cost_estimate=pl.CostEstimate(
            flops=12 * rows * half * units, transcendentals=rows * units, bytes_accessed=12 * half * units
        ),
        name="ffn",
    )(side, gain_m, gain_t, w_gate, w_up, w_down, *pieces_in)


def keep_body(wg, wu, wd, *refs):
    refs[-1][...] = refs[0][...]


def keep(value, *weights):
    vm = pl.BlockSpec(memory_space=pltpu.VMEM)
    return pl.pallas_call(
        keep_body,
        out_shape=jax.ShapeDtypeStruct(value.shape, value.dtype),
        in_specs=[vm] * 4,
        out_specs=vm,
        compiler_params=pltpu.CompilerParams(vmem_limit_bytes=16 * MIB),
        name="keep",
    )(*weights, value)


def tail_body(tgt_ref, wts_ref, *refs, places):
    rows, out = refs[: len(places)], refs[-1]
    tok_count = tgt_ref.shape[1]
    total = refs[len(places)][...] if len(refs) > len(places) + 1 else None
    for j in range(2):
        picked = None
        for at, ref in zip(places, rows):
            row = lax.broadcasted_iota(jnp.int32, (ref.shape[0], tok_count), 0) + at
            pick = (tgt_ref[j : j + 1, :] == row).astype(jnp.float32).astype(jnp.bfloat16)
            part = lax.dot_general(
                pick, ref[...], (((0,), (0,)), ((), ())), preferred_element_type=jnp.float32
            )
            picked = part if picked is None else picked + part
        part = picked * wts_ref[:, j : j + 1]
        total = part if total is None else total + part
    out[...] = total


def tail(targets, weights, rows, *total):
    tok_count = targets.shape[1]
    vm = pl.BlockSpec(memory_space=pltpu.VMEM)
    return pl.pallas_call(
        functools.partial(tail_body, places=tuple(at for at, _ in rows)),
        out_shape=jax.ShapeDtypeStruct((tok_count, rows[0][1].shape[1]), jnp.float32),
        in_specs=[vm] * (2 + len(rows) + len(total)),
        out_specs=vm,
        compiler_params=pltpu.CompilerParams(vmem_limit_bytes=12 * MIB),
        name="tail",
    )(targets, weights, *[r for _, r in rows], *total)


def per_device(tokens, in_gain, route_ids, route_weights, w_gate, w_up, w_down, out_gain):
    tok_count, half = tokens.shape
    ep_size = lax.axis_size("ep")
    tp_size = lax.axis_size("tp")
    experts = ep_size // SPAN_EP
    capacity = 2 * (5 * tok_count // (4 * experts))
    home = (lax.axis_index("ep") // SPAN_EP).astype(jnp.int32)
    side = lax.axis_index("tp").astype(jnp.int32).reshape(1)
    swap = [(i, i ^ 1) for i in range(tp_size)]

    def tp_swap(v):
        return lax.ppermute(v, "tp", swap)

    def member_swap(v):
        return lax.ppermute(v, "ep", [(i, i ^ 1) for i in range(ep_size)])

    def hop(v, k, back=False):
        if k == 0:
            return v
        pairs = [
            (e * SPAN_EP + i, away(e, k, experts) * SPAN_EP + i) for e in range(experts) for i in range(SPAN_EP)
        ]
        return lax.ppermute(v, "ep", [(b, a) for a, b in pairs] if back else pairs)

    gain_m = in_gain.reshape(1, half)
    apart = capacity % 32 == 0
    gain_t = tp_swap(gain_m)
    cut_in = [sizes_of(capacity, apart and 2 * k == experts) for k in range(experts)]
    cut_back = [sizes_of(capacity, apart and 2 * k >= experts) for k in range(experts)]
    flat = [size for sizes in cut_in for size in sizes]
    targets, *sent = front(home.reshape(1), route_ids.T, tokens, experts, capacity, flat)
    weights = (w_gate, w_up, w_down)
    gain_m = keep(gain_m, *weights)
    gain_r = keep(gain_m, *weights)
    results = []
    for k in range(experts):
        near = []
        for _ in range(len(cut_in[k])):
            piece = sent.pop(0)
            near.append(hop(piece, k))
        crossed = []
        for piece in near:
            crossed.append(member_swap(piece))
        mine = near + crossed
        theirs = []
        for piece in mine:
            theirs.append(tp_swap(piece))
        if k == 0:
            own, other = ffn(side, mine + theirs, gain_m, gain_t, *weights)
        else:
            own, other = resident_ffn(side, mine + theirs, gain_r, gain_t, *weights)
        back = tp_swap(other)
        pair = (own.astype(jnp.float32) + back.astype(jnp.float32)).astype(jnp.bfloat16)
        kept = pieces(pair[:capacity], cut_back[k])
        for p, piece in enumerate(pieces(pair[capacity:], cut_back[k])):
            cross = member_swap(piece)
            result = (kept[p].astype(jnp.float32) + cross.astype(jnp.float32)).astype(jnp.bfloat16)
            results.append((k * capacity + sum(cut_back[k][:p]), hop(result, k, True)))
    middle = experts // 2 * capacity
    early = [r for r in results if r[0] >= middle]
    late = [r for r in results if r[0] < middle]
    combined = tail(targets, route_weights, early)
    combined = tail(targets, route_weights, late, combined)
    second_sum = lax.psum(jnp.sum(combined * combined, axis=1), "tp")
    return (combined * lax.rsqrt(second_sum[:, None] / (tp_size * half) + EPS) * out_gain[None, :]).astype(jnp.bfloat16)


def solution(mesh):
    placed = (
        P(("grp", "ep"), "tp"),
        P("tp"),
        P(("grp", "ep"), None),
        P(("grp", "ep"), None),
        P("ep", None, "tp"),
        P("ep", None, "tp"),
        P("ep", "tp", None),
        P("tp"),
    )
    return jax.shard_map(
        per_device, mesh=mesh, in_specs=placed, out_specs=P(("grp", "ep"), "tp"), check_vma=False
    )
```
